32 devices in a mesh: fs: 32 (over z, y, x, core), tp: 1.
Axes of the slice: x: 2, y: 2, z: 4, core: 2. Of those that a mesh axis runs over, the one named last changes fastest.
Arguments:
- later_input: bfloat16 [6144, 2048], P(('fs', 'tp')), may hold values from -6 to 6
- earlier_input: bfloat16 [6144, 2048], P(('fs', 'tp')), may hold values from -6 to 6
- cotangent: bfloat16 [6144, 2048], P(('fs', 'tp')), may hold values from -6 to 6
- gate_weight: bfloat16 [2048, 3072], P('fs', 'tp'), may hold values from -0.125 to 0.125
- up_weight: bfloat16 [2048, 3072], P('fs', 'tp'), may hold values from -0.125 to 0.125
- down_weight: bfloat16 [2048, 3072], P('fs', 'tp'), may hold values from -0.109375 to 0.109375
- down_grad_sum: float32 [2048, 3072], P('fs', 'tp'), may hold values from -6 to 6
Outputs:
- later_output: bfloat16 [6144, 2048], P(('fs', 'tp'))
- earlier_grad_input: bfloat16 [6144, 2048], P(('fs', 'tp'))
- new_down_grad_sum: float32 [2048, 3072], P('fs', 'tp')
The draws below stay inside these ranges and needn't reach their ends.
All inputs are finite; a program needn't handle non-finite values.
Results may differ from the reference program's by a relative error of at most 0.0057.
Values may be sent and summed in bfloat16 or wider, within the bound.
A program may use at most 192 MiB of HBM per device.

```python
import jax
import jax.numpy as jnp
from jax import lax

D = 2048
FF = 3072
TOKENS = 6144
N_TP = 1


def raised(result, key, source, target, blocks, factor):
    owner, partner = [(jnp.arange(result.shape[axis_at]) // (result.shape[axis_at] // blocks)).reshape([-1 if axis == axis_at else 1 for axis in range(result.ndim)]) for axis_at in (source, target)]
    chosen = jax.random.permutation(key, blocks)[partner]
    strong = (owner == chosen) | (owner == (partner + blocks // 2) % blocks)
    return jnp.where(strong, factor * result, result)


def block_scale(rng, shape, split, low, top_value):
    factor_of, own = 1.0, jax.random.fold_in(rng, 6)
    for position, parts in split:
        heights = jnp.exp(jax.random.uniform(jax.random.fold_in(own, position), (parts,), jnp.float32, low / len(split), top_value / len(split)))
        factor_of = factor_of * jnp.repeat(heights, shape[position] // parts).reshape([-1 if axis == position else 1 for axis in range(len(shape))])
    return factor_of


def noise(stream_key, dims, deviation, most, shards=(), kind=jnp.bfloat16):
    loudness = block_scale(stream_key, dims, shards, -0.22, 0.18) if shards else 1.0
    entries = jax.random.normal(stream_key, dims, jnp.float32) * deviation * loudness
    return jnp.minimum(jnp.maximum(entries, -most), most).astype(kind)


def bell_draw_with(own_key, dims, deviation, most, split, heavy, held_as=jnp.bfloat16):
    entries = deviation * jax.random.normal(own_key, dims, jnp.float32)
    if split:
        entries = entries * block_scale(own_key, dims, split, -0.22, 0.18)
    return jnp.clip(raised(entries, jax.random.fold_in(own_key, 3), *heavy), -most, most).astype(held_as)


def setup_inputs(seed: int = 0) -> dict:
    keys = jax.random.split(jax.random.key(seed), 8)
    later_input = noise(keys[0], (TOKENS, D), 1.0, 6.0, ((0, 32),))
    earlier_input = noise(keys[1], (TOKENS, D), 1.0, 6.0, ((0, 32),))
    cotangent = bell_draw_with(keys[2], (TOKENS, D), 1.0, 6.0, ((0, 32),), (0, 1, 32, 2.75))
    gate_weight = noise(keys[3], (D, FF), D ** -0.5, 0.125, ((0, 32),))
    up_weight = noise(keys[4], (D, FF), D ** -0.5, 0.125, ((0, 32),))
    down_weight = noise(keys[5], (D, FF), FF ** -0.5, 0.109375, ((0, 32),))
    down_grad_sum = noise(keys[6], (D, FF), 1.0, 6.0, ((0, 32),), jnp.float32)
    return dict(later_input=later_input, earlier_input=earlier_input, cotangent=cotangent, gate_weight=gate_weight, up_weight=up_weight, down_weight=down_weight, down_grad_sum=down_grad_sum)


def partial_rows(gradients, weights, first_unit, last_unit):
    return jnp.dot(gradients[:, first_unit:last_unit], weights[:, first_unit:last_unit].T, preferred_element_type=jnp.float32)


def rounded_sum(total, partial_value):
    kept = lax.optimization_barrier(partial_value.astype(jnp.bfloat16))
    return total + kept.astype(jnp.float32)


def reference(later_input, earlier_input, cotangent, gate_weight, up_weight, down_weight, down_grad_sum):
    block_width = FF // N_TP
    gate_later = jnp.dot(later_input, gate_weight, preferred_element_type=jnp.float32)
    up_later = jnp.dot(later_input, up_weight, preferred_element_type=jnp.float32)
    hidden_later = (jax.nn.silu(gate_later) * up_later).astype(jnp.bfloat16)
    output_total = jnp.zeros((TOKENS, D), jnp.float32)
    for block_index in range(N_TP):
        first_unit = block_index * block_width
        partial_value = partial_rows(hidden_later, down_weight, first_unit, first_unit + block_width)
        output_total = rounded_sum(output_total, partial_value)
    later_output = output_total.astype(jnp.bfloat16)

    gate_early = jnp.dot(earlier_input, gate_weight, preferred_element_type=jnp.float32)
    up_early = jnp.dot(earlier_input, up_weight, preferred_element_type=jnp.float32)
    sigmoid_gate = jax.nn.sigmoid(gate_early)
    activated = gate_early * sigmoid_gate
    hidden_early = (activated * up_early).astype(jnp.bfloat16)
    grad_hidden = jnp.dot(cotangent, down_weight, preferred_element_type=jnp.float32)
    grad_gate = (grad_hidden * up_early * sigmoid_gate * (1.0 + gate_early * (1.0 - sigmoid_gate))).astype(jnp.bfloat16)
    grad_up = (grad_hidden * activated).astype(jnp.bfloat16)
    input_total = jnp.zeros((TOKENS, D), jnp.float32)
    for block_index in range(N_TP):
        first_unit = block_index * block_width
        last_unit = first_unit + block_width
        partial_value = partial_rows(grad_gate, gate_weight, first_unit, last_unit) + partial_rows(grad_up, up_weight, first_unit, last_unit)
        input_total = rounded_sum(input_total, partial_value)
    earlier_grad_input = input_total.astype(jnp.bfloat16)

    weight_grad = jnp.dot(cotangent.T, hidden_early, preferred_element_type=jnp.float32)
    new_down_grad_sum = down_grad_sum + weight_grad * (TOKENS ** -0.5)
    return (later_output, earlier_grad_input, new_down_grad_sum)
```

```python
import functools

import jax
import jax.numpy as jnp
from jax import lax
from jax.experimental import pallas as pl
from jax.experimental.pallas import tpu as pltpu
from jax.sharding import PartitionSpec as P

QUAD = 4


def contract_last(leading, trailing):
    return lax.dot_general(
        leading, trailing, (((1,), (1,)), ((), ())), preferred_element_type=jnp.float32
    )


def add_parts(received, group):
    pieces = received.reshape(group, received.shape[0] // group, received.shape[1])
    return jnp.sum(pieces.astype(jnp.float32), axis=0).astype(jnp.bfloat16)


def shards(
    later_input, earlier_input, cotangent, gate_weight, up_weight, down_weight, down_grad_sum
):
    group = lax.axis_size("tp")
    later_rows, early_rows, grad_rows = (
        lax.all_gather(later_input, "tp", axis=0, tiled=True),
        lax.all_gather(earlier_input, "tp", axis=0, tiled=True),
        lax.all_gather(cotangent, "tp", axis=0, tiled=True),
    )
    columns = later_rows
    gate_later = jnp.dot(
        columns,
        lax.all_gather(gate_weight, "fs", axis=0, tiled=True),
        preferred_element_type=jnp.float32,
    )
    up_later = jnp.dot(
        columns,
        lax.all_gather(up_weight, "fs", axis=0, tiled=True),
        preferred_element_type=jnp.float32,
    )
    hidden_later = (jax.nn.silu(gate_later) * up_later).astype(jnp.bfloat16)
    partials = contract_last(hidden_later, lax.all_gather(down_weight, "fs", axis=0, tiled=True))
    gate_whole, up_whole, down_whole = (
        lax.all_gather(gate_weight, "fs", axis=0, tiled=True),
        lax.all_gather(up_weight, "fs", axis=0, tiled=True),
        lax.all_gather(down_weight, "fs", axis=0, tiled=True),
    )
    output_received = lax.all_to_all(
        partials.astype(jnp.bfloat16), "tp", split_axis=0, concat_axis=0, tiled=True
    )
    later_output = add_parts(output_received, group)
    gate_early = jnp.dot(early_rows, gate_whole, preferred_element_type=jnp.float32)
    up_early = jnp.dot(early_rows, up_whole, preferred_element_type=jnp.float32)
    sigmoid_gate = jax.nn.sigmoid(gate_early)
    activated = gate_early * sigmoid_gate
    hidden_early = (activated * up_early).astype(jnp.bfloat16)
    grad_hidden = jnp.dot(grad_rows, down_whole, preferred_element_type=jnp.float32)
    grad_gate = (
        grad_hidden * up_early * sigmoid_gate * (1.0 + gate_early * (1.0 - sigmoid_gate))
    ).astype(jnp.bfloat16)
    grad_up = (grad_hidden * activated).astype(jnp.bfloat16)
    input_partial = contract_last(grad_gate, gate_whole) + contract_last(grad_up, up_whole)
    input_received = lax.all_to_all(
        input_partial.astype(jnp.bfloat16), "tp", split_axis=0, concat_axis=0, tiled=True
    )
    earlier_grad_input = add_parts(input_received, group)
    columns = grad_rows
    summed = lax.psum_scatter(
        lax.dot_general(
            columns, hidden_early, (((0,), (0,)), ((), ())), preferred_element_type=jnp.float32
        ),
        "fs",
        scatter_dimension=0,
        tiled=True,
    )
    factor = (later_rows.shape[0] * lax.axis_size("fs")) ** (-0.5)
    return (later_output, earlier_grad_input, down_grad_sum + summed * factor)

def ring_group(place, ring):
    half = lax.div(2 * place, ring)
    return 2 * place * (1 - half) + (2 * (ring - 1 - place) + 1) * half


def ring_place(group, ring):
    odd = lax.rem(group, 2)
    return lax.div(group, 2) * (1 - odd) + (ring - 1 - lax.div(group, 2)) * odd


def fused_kernel(ring, factor, *refs):
    token_refs, weight_refs, sum_ref = refs[:3], refs[3:6], refs[6]
    outs, sum_out = refs[7:9], refs[9]
    whole, tok, acc, mine, near_send, near_recv, far_send, far_recv, travel, trade_send, trade_recv = refs[10:21]
    (quad_ss, quad_rs, first_ss, first_rs, ring_ss, ring_rs, tok_ss, tok_rs, near_ss, near_rs,
     far_ss, far_rs, sum_ss, sum_rs, trade_ss, trade_rs, local_sem) = refs[21:]
    bf16, f32 = jnp.bfloat16, jnp.float32
    me = lax.axis_index("fs")
    group, lane = lax.div(me, QUAD), lax.rem(me, QUAD)
    low, high = lax.rem(lane, 2), lax.div(lane, 2)
    relative = [lane, lane + 1 - 2 * low, lane + 2 - 4 * high, QUAD - 1 - lane]
    peers = [group * QUAD + other for other in relative]
    place = ring_place(group, ring)

    def group_at(shift):
        return ring_group(lax.rem(place + shift + ring, ring), ring)

    around = [group_at(1) * QUAD + lane, group_at(-1) * QUAD + lane]
    depth = weight_refs[0].shape[0]
    width = whole.shape[2]
    chunk, half = QUAD * depth, 2 * depth
    rows = token_refs[0].shape[0]
    total_rows = tok.shape[1]
    reach = ring // 2
    per_slab = total_rows // chunk
    halves = [[high, 1 - high], [1 - high, high]]

    barrier = pltpu.get_barrier_semaphore()
    for other in peers[1:] + around:
        pl.semaphore_signal(
            barrier, inc=1, device_id={"fs": other}, device_id_type=pl.DeviceIdType.MESH
        )
    pl.semaphore_wait(barrier, QUAD + 1)

    def remote(source, target, send, recv, other):
        return pltpu.make_async_remote_copy(
            src_ref=source,
            dst_ref=target,
            send_sem=send,
            recv_sem=recv,
            device_id={"fs": other},
            device_id_type=pl.DeviceIdType.MESH,
        )

    def slab(weight, owner, member):
        first = pl.multiple_of((owner * QUAD + member) * depth, depth)
        return whole.at[weight, pl.ds(first, depth), :]

    def columns(weight, member):
        return weight_refs[weight].at[:, pl.ds(pl.multiple_of(member * width, width), width)]

    def half_slab(weight, owner, part):
        first = pl.multiple_of(owner * chunk + part * half, half)
        return whole.at[weight, pl.ds(first, half), :]

    sent, kept = [], []

    def begin(copy):
        copy.start()
        sent.append(copy)
        return copy

    quad, first_hop, hop, tokens = {}, {}, {}, {}
    for weight in range(3):
        for far in (1, 3, 2):
            quad[weight, far] = begin(
                remote(
                    columns(weight, relative[far]),
                    slab(weight, group, lane),
                    quad_ss.at[weight, far - 1],
                    quad_rs.at[weight, far - 1],
                    peers[far],
                )
            )

    def hop_first(weight, piece):
        for way in range(2):
            target = slab(weight, group, relative[piece])
            first_hop[weight, way, piece] = begin(
                remote(
                    columns(weight, lane) if piece == 0 else target,
                    target,
                    first_ss.at[weight, way, piece],
                    first_rs.at[weight, way, piece],
                    around[way],
                )
            )

    hop_first(0, 0)
    hop_first(1, 0)
    for weight in range(3):
        copy = pltpu.make_async_copy(
            columns(weight, lane), slab(weight, group, lane), local_sem.at[weight]
        )
        copy.start()
        kept.append(copy)

    def row_block(token, block):
        return tok.at[token, pl.ds(block * rows, rows), :]

    def send_rows(token, source, block, slot, other):
        tokens[token, slot] = begin(
            remote(
                source,
                row_block(token, block),
                tok_ss.at[token, slot],
                tok_rs.at[token, slot],
                other,
            )
        )

    for token in range(3):
        send_rows(token, token_refs[token], 2, 1, peers[2])
        send_rows(token, token_refs[token], 1, 0, peers[1])
        copy = pltpu.make_async_copy(
            token_refs[token], row_block(token, 0), local_sem.at[3 + token]
        )
        copy.start()
        kept.append(copy)

    def clear(index, carry):
        acc[index] = jnp.zeros(acc.shape[1:], f32)
        return carry

    lax.fori_loop(0, 4, clear, 0)
    acc[acc.shape[0] - 1] = jnp.zeros(acc.shape[1:], f32)

    for weight in (0, 1):
        quad[weight, 1].wait_recv()
        hop_first(weight, 1)
    hop_first(2, 0)
    quad[2, 1].wait_recv()
    hop_first(2, 1)
    for weight in range(3):
        for piece in (3, 2):
            quad[weight, piece].wait_recv()
            hop_first(weight, piece)
    for copy in kept:
        copy.wait()

    arrived = set()

    def arrival(weight, way, step, order):
        if (weight, way, step, order) in arrived:
            return
        arrived.add((weight, way, step, order))
        if step == 1:
            own_half = (order == 0) == (way == 0)
            for piece in (0, 1) if own_half else (3, 2):
                first_hop[weight, way, piece].wait_recv()
        else:
            hop[weight, way, step, order].wait_recv()

    def forward(weight, step, order):
        for way in range(2):
            arrival(weight, way, step - 1, order)
            shift = (1 - step) if way == 0 else (step - 1)
            part = half_slab(weight, group_at(shift), halves[way][order])
            hop[weight, way, step, order] = begin(
                remote(
                    part,
                    part,
                    ring_ss.at[weight, way, step - 2, order],
                    ring_rs.at[weight, way, step - 2, order],
                    around[way],
                )
            )

    def arrive(weight, distance):
        for way in range(2):
            for order in range(1 if distance == reach else 2):
                arrival(weight, way, distance, order)

    def token_over(token):
        tokens[token, 1].wait_recv()
        send_rows(token, row_block(token, 2), 3, 2, peers[1])

    def token_in(token):
        tokens[token, 0].wait_recv()
        tokens[token, 2].wait_recv()

    def span(owner):
        return pl.ds(pl.multiple_of(owner * chunk, chunk), chunk)

    def project(token, shift):
        where = span(group_at(shift))
        left = tok[token, :, where]
        for weight in range(2):
            slot = 2 * token + weight
            acc[slot] += jnp.dot(left, whole[weight, where, :], preferred_element_type=f32)

    def loop(first, last, body):
        def step(index, carry):
            body(index)
            return carry

        lax.fori_loop(first, last, step, 0)

    def project_pair(distance, token_list):
        if distance == reach:
            loop(0, len(token_list), lambda i: project(token_list[0] + i, reach))
        else:
            loop(
                0,
                2 * len(token_list),
                lambda i: project(
                    token_list[0] + lax.div(i, 2), (2 * lax.rem(i, 2) - 1) * distance
                ),
            )

    for order in range(2):
        for weight in (0, 1):
            forward(weight, 2, order)
    token_over(0)
    token_in(0)
    loop(0, 3, lambda i: project(0, i - 1))
    later_started = False
    for step in range(3, reach + 1):
        last = step == reach
        if last:
            token_over(1)
            token_in(1)
            loop(0, 3, lambda i: project(1, i - 1))
            for distance in range(2, reach - 1):
                project_pair(distance, [1])
        for order in range(1 if last else 2):
            for weight in (0, 1):
                forward(weight, step, order)
        if last:
            for order in range(2):
                forward(2, 2, order)
        for weight in (0, 1):
            arrive(weight, step - 1)
        project_pair(step - 1, [0, 1] if last else [0])
    token_over(2)
    for weight in (0, 1):
        arrive(weight, reach)
    project_pair(reach, [0, 1])
    for token in range(2):
        for slot in range(3):
            tokens[token, slot].wait_send()
            sent[:] = [copy for copy in sent if copy is not tokens[token, slot]]

    tile = 32

    def early_values(index):
        where = pl.ds(pl.multiple_of(index * tile, tile), tile)
        gate, up = acc[0, where, :], acc[1, where, :]
        sig = jax.nn.sigmoid(gate)
        act = gate * sig
        tok[0, where, 0:width] = (act * up).astype(bf16)
        acc[0, where, :] = up * sig * (1.0 + gate * (1.0 - sig))
        acc[1, where, :] = act

    def later_values(index):
        where = pl.ds(pl.multiple_of(index * tile, tile), tile)
        gate, up = acc[2, where, :], acc[3, where, :]
        tok[1, where, 0:width] = (gate * jax.nn.sigmoid(gate) * up).astype(bf16)

    loop(0, total_rows // tile, early_values)
    forward(2, 3, 0)
    loop(0, total_rows // tile, later_values)
    token_in(2)

    def slab_of(index):
        if isinstance(index, int):
            return 2 + index // per_slab, index % per_slab * chunk
        first = pl.multiple_of(lax.rem(index, per_slab) * chunk, chunk)
        return 2 + lax.div(index, per_slab), first

    def partial_sum(index):
        left = tok[2, :, span(group_at(index))]
        place_of, first = slab_of(index)
        acc[place_of, pl.ds(first, chunk), :] = lax.dot_general(
            left, tok[0, :, 0:width], (((0,), (0,)), ((), ())), preferred_element_type=f32
        )

    def own_part(shift, part):
        place_of, first = slab_of((shift + ring) % ring)
        return acc[place_of, pl.ds(pl.multiple_of(first + part * half, half), half), :]

    def near_copy(which, owner):
        return remote(
            near_send.at[which, owner],
            near_recv.at[which, owner],
            near_ss.at[which, owner],
            near_rs.at[which, owner],
            peers[1],
        )

    def far_copy(which, owner):
        return remote(
            far_send.at[which, owner],
            far_recv.at[which, owner],
            far_ss.at[which, owner],
            far_rs.at[which, owner],
            peers[2],
        )

    def produce(which, owner, value):
        mine[which, owner, 0] = value[:rows]
        mine[which, owner, 1] = value[2 * rows : 3 * rows]
        near_send[which, owner, 0] = value[rows : 2 * rows].astype(bf16)
        near_send[which, owner, 1] = value[3 * rows :].astype(bf16)
        near_copy(which, owner).start()

    def relay(which, owner):
        near_copy(which, owner).wait_recv()
        mine[which, owner, 0] += near_recv[which, owner, 0].astype(f32)
        far_send[which, owner] = (
            mine[which, owner, 1] + near_recv[which, owner, 1].astype(f32)
        ).astype(bf16)
        far_copy(which, owner).start()

    def finish(which, owner):
        far_copy(which, owner).wait_recv()
        outs[which][:, span(owner)] = (
            mine[which, owner, 0] + far_recv[which, owner].astype(f32)
        ).astype(bf16)

    last_slab = acc.shape[0] - 1

    def down_step(shift):
        owner = group_at(shift)
        where = span(owner)
        right = whole[2, where, :]
        produce(0, owner, contract_last(tok[1, :, 0:width], right))
        acc[last_slab] += jnp.dot(tok[2, :, where], right, preferred_element_type=f32)

    loop(0, 3, lambda i: down_step(i - 1))
    forward(2, 3, 1)
    loop(0, 3, lambda i: relay(0, group_at(i - 1)))
    loop(0, ring, partial_sum)

    for step in range(3, reach + 1):
        if step > 3:
            for order in range(1 if step == reach else 2):
                forward(2, step, order)
        arrive(2, step - 1)
        distance = step - 1
        loop(0, 2, lambda i: down_step((2 * i - 1) * distance))
        loop(0, 2, lambda i: relay(0, group_at((2 * i - 1) * distance)))

    moved = {}

    def pass_on(step, order, add):
        for way in range(2):
            part = halves[way][1 - order]
            shift = (reach + 1 - step) * (1 if way == 0 else -1)
            if add:
                moved[way, step - 1, order].wait_recv()
                travel[way, step - 1, order] = (
                    travel[way, step - 1, order].astype(f32) + own_part(shift, part)
                ).astype(bf16)
            else:
                travel[way, step - 1, order] = own_part(shift, part).astype(bf16)
        for way in range(2):
            moved[way, step, order] = begin(
                remote(
                    travel.at[way, step - 1, order],
                    travel.at[way, step, order],
                    sum_ss.at[way, step - 1, order],
                    sum_rs.at[way, step - 1, order],
                    around[way],
                )
            )

    pass_on(1, 1, False)
    pass_on(2, 0, False)
    arrive(2, reach)
    down_step(reach)

    def grads(index):
        where = pl.ds(pl.multiple_of(index * tile, tile), tile)
        hidden = acc[last_slab, where, :]
        tok[0, where, width : 2 * width] = (hidden * acc[0, where, :]).astype(bf16)
        tok[1, where, width : 2 * width] = (hidden * acc[1, where, :]).astype(bf16)

    loop(0, total_rows // tile, grads)
    relay(0, group_at(reach))

    def input_step(owner):
        where = span(owner)
        produce(
            1,
            owner,
            contract_last(tok[0, :, width : 2 * width], whole[0, where, :])
            + contract_last(tok[1, :, width : 2 * width], whole[1, where, :]),
        )

        @pl.when(owner > 0)
        def _():
            relay(1, owner - 1)

    pauses = [(2, 1)] + [(step, order) for step in range(3, reach + 1) for order in (0, 1)]
    stops = [ring // 4, ring // 2 + 1, ring]
    first = 0
    for stop in stops:
        loop(first, stop, input_step)
        first = stop
        if pauses:
            pass_on(*pauses.pop(0), True)
    relay(1, ring - 1)
    loop(0, ring, lambda i: finish(0, i))
    while pauses:
        pass_on(*pauses.pop(0), True)
    loop(0, ring, lambda i: finish(1, i))

    def total_of(part, order_pair):
        for way in range(2):
            moved[way, reach, order_pair[way]].wait_recv()
        return (
            own_part(0, part)
            + travel[0, reach, order_pair[0]].astype(f32)
            + travel[1, reach, order_pair[1]].astype(f32)
        )

    def order_of(way, own):
        return 1 - (0 if (way == 0) == own else 1)

    far_pair = [order_of(0, False), order_of(1, False)]
    near_pair = [order_of(0, True), order_of(1, True)]

    def trade(piece, member):
        first = pl.multiple_of(member * depth, depth)
        return begin(
            remote(
                trade_send.at[pl.ds(first, depth), :],
                trade_recv.at[piece - 1],
                trade_ss.at[piece - 1],
                trade_rs.at[piece - 1],
                peers[piece],
            )
        )

    far_rows = pl.ds(pl.multiple_of((1 - high) * half, half), half)
    near_rows = pl.ds(pl.multiple_of(high * half, half), half)
    trade_send[far_rows, :] = total_of(1 - high, far_pair).astype(bf16)
    trades = {piece: trade(piece, relative[piece]) for piece in (2, 3)}
    own_sum = total_of(high, near_pair)
    trade_send[near_rows, :] = own_sum.astype(bf16)
    trades[1] = trade(1, relative[1])
    place_of, first = slab_of(0)
    acc[place_of, pl.ds(pl.multiple_of(first + high * half, half), half), :] = own_sum

    def across(member):
        return pl.ds(pl.multiple_of(member * width, width), width)

    own_rows = pl.ds(pl.multiple_of(first + lane * depth, depth), depth)
    sum_out[:, across(lane)] = sum_ref[:, across(lane)] + acc[place_of, own_rows, :] * factor
    for piece in (1, 2, 3):
        trades[piece].wait_recv()
        there = across(relative[piece])
        sum_out[:, there] = sum_ref[:, there] + trade_recv[piece - 1].astype(f32) * factor

    for copy in sent:
        copy.wait_send()

    def drain(index):
        which, owner = lax.div(index, ring), lax.rem(index, ring)
        near_copy(which, owner).wait_send()
        far_copy(which, owner).wait_send()

    loop(0, 2 * ring, drain)


def fused_shards(
    later_input, earlier_input, cotangent, gate_weight, up_weight, down_weight, down_grad_sum
):
    ring = lax.axis_size("fs") // QUAD
    rows, model = later_input.shape
    depth, hidden = gate_weight.shape
    width, chunk, total_rows = hidden // QUAD, QUAD * depth, QUAD * rows
    reach = ring // 2
    slabs = 2 + max(2, pl.cdiv(ring, total_rows // chunk)) + 1
    dma = pltpu.SemaphoreType.DMA
    bf16, f32 = jnp.bfloat16, jnp.float32
    vmem, anywhere = pl.BlockSpec(memory_space=pltpu.VMEM), pl.BlockSpec(memory_space=pl.ANY)
    factor = (rows * lax.axis_size("fs")) ** (-0.5)
    return tuple(
        pl.pallas_call(
            functools.partial(fused_kernel, ring, factor),
            out_shape=[
                jax.ShapeDtypeStruct(later_input.shape, bf16),
                jax.ShapeDtypeStruct(earlier_input.shape, bf16),
                jax.ShapeDtypeStruct(down_grad_sum.shape, f32),
            ],
            in_specs=[anywhere] * 3 + [vmem] * 4,
            out_specs=[vmem] * 3,
            scratch_shapes=[
                pltpu.VMEM((3, model, width), bf16),
                pltpu.VMEM((3, total_rows, model), bf16),
                pltpu.VMEM((slabs, total_rows, width), f32),
                pltpu.VMEM((2, ring, 2, rows, chunk), f32),
                pltpu.VMEM((2, ring, 2, rows, chunk), bf16),
                pltpu.VMEM((2, ring, 2, rows, chunk), bf16),
                pltpu.VMEM((2, ring, rows, chunk), bf16),
                pltpu.VMEM((2, ring, rows, chunk), bf16),
                pltpu.VMEM((2, reach + 1, 2, 2 * depth, width), bf16),
                pltpu.VMEM((chunk, width), bf16),
                pltpu.VMEM((3, depth, width), bf16),
                dma((3, 3)),
                dma((3, 3)),
                dma((3, 2, QUAD)),
                dma((3, 2, QUAD)),
                dma((3, 2, reach - 1, 2)),
                dma((3, 2, reach - 1, 2)),
                dma((3, 3)),
                dma((3, 3)),
                dma((2, ring)),
                dma((2, ring)),
                dma((2, ring)),
                dma((2, ring)),
                dma((2, reach, 2)),
                dma((2, reach, 2)),
                dma((3,)),
                dma((3,)),
                dma((6,)),
            ],
            compiler_params=pltpu.CompilerParams(
                collective_id=0, has_side_effects=True, vmem_limit_bytes=67_043_328
            ),
        )(
            earlier_input,
            later_input,
            cotangent,
            gate_weight,
            up_weight,
            down_weight,
            down_grad_sum,
        )
    )


def fits(mesh):
    return mesh.shape["tp"] == 1 and mesh.shape["fs"] == 8 * QUAD


def solution(mesh):
    in_specs = (
        P(("fs", "tp"), None),
        P(("fs", "tp"), None),
        P(("fs", "tp"), None),
        P("fs", "tp"),
        P("fs", "tp"),
        P("fs", "tp"),
        P("fs", "tp"),
    )
    out_specs = (P(("fs", "tp"), None), P(("fs", "tp"), None), P("fs", "tp"))
    body = fused_shards if fits(mesh) else shards
    return jax.shard_map(body, mesh=mesh, in_specs=in_specs, out_specs=out_specs, check_vma=False)
```

```python
import functools

import jax
import jax.numpy as jnp
from jax import lax
from jax.experimental import pallas as pl
from jax.experimental.pallas import tpu as pltpu
from jax.sharding import PartitionSpec as P

QUAD = 4


def contract_last(leading, trailing):
    return lax.dot_general(
        leading, trailing, (((1,), (1,)), ((), ())), preferred_element_type=jnp.float32
    )


def add_parts(received, group):
    pieces = received.reshape(group, received.shape[0] // group, received.shape[1])
    return jnp.sum(pieces.astype(jnp.float32), axis=0).astype(jnp.bfloat16)


def shards(
    later_input, earlier_input, cotangent, gate_weight, up_weight, down_weight, down_grad_sum
):
    group = lax.axis_size("tp")
    later_rows, early_rows, grad_rows = (
        lax.all_gather(later_input, "tp", axis=0, tiled=True),
        lax.all_gather(earlier_input, "tp", axis=0, tiled=True),
        lax.all_gather(cotangent, "tp", axis=0, tiled=True),
    )
    columns = later_rows
    gate_later = jnp.dot(
        columns,
        lax.all_gather(gate_weight, "fs", axis=0, tiled=True),
        preferred_element_type=jnp.float32,
    )
    up_later = jnp.dot(
        columns,
        lax.all_gather(up_weight, "fs", axis=0, tiled=True),
        preferred_element_type=jnp.float32,
    )
    hidden_later = (jax.nn.silu(gate_later) * up_later).astype(jnp.bfloat16)
    partials = contract_last(hidden_later, lax.all_gather(down_weight, "fs", axis=0, tiled=True))
    gate_whole, up_whole, down_whole = (
        lax.all_gather(gate_weight, "fs", axis=0, tiled=True),
        lax.all_gather(up_weight, "fs", axis=0, tiled=True),
        lax.all_gather(down_weight, "fs", axis=0, tiled=True),
    )
    output_received = lax.all_to_all(
        partials.astype(jnp.bfloat16), "tp", split_axis=0, concat_axis=0, tiled=True
    )
    later_output = add_parts(output_received, group)
    gate_early = jnp.dot(early_rows, gate_whole, preferred_element_type=jnp.float32)
    up_early = jnp.dot(early_rows, up_whole, preferred_element_type=jnp.float32)
    sigmoid_gate = jax.nn.sigmoid(gate_early)
    activated = gate_early * sigmoid_gate
    hidden_early = (activated * up_early).astype(jnp.bfloat16)
    grad_hidden = jnp.dot(grad_rows, down_whole, preferred_element_type=jnp.float32)
    grad_gate = (
        grad_hidden * up_early * sigmoid_gate * (1.0 + gate_early * (1.0 - sigmoid_gate))
    ).astype(jnp.bfloat16)
    grad_up = (grad_hidden * activated).astype(jnp.bfloat16)
    input_partial = contract_last(grad_gate, gate_whole) + contract_last(grad_up, up_whole)
    input_received = lax.all_to_all(
        input_partial.astype(jnp.bfloat16), "tp", split_axis=0, concat_axis=0, tiled=True
    )
    earlier_grad_input = add_parts(input_received, group)
    columns = grad_rows
    summed = lax.psum_scatter(
        lax.dot_general(
            columns, hidden_early, (((0,), (0,)), ((), ())), preferred_element_type=jnp.float32
        ),
        "fs",
        scatter_dimension=0,
        tiled=True,
    )
    factor = (later_rows.shape[0] * lax.axis_size("fs")) ** (-0.5)
    return (later_output, earlier_grad_input, down_grad_sum + summed * factor)

def ring_group(place, ring):
    half = lax.div(2 * place, ring)
    return 2 * place * (1 - half) + (2 * (ring - 1 - place) + 1) * half


def ring_place(group, ring):
    odd = lax.rem(group, 2)
    return lax.div(group, 2) * (1 - odd) + (ring - 1 - lax.div(group, 2)) * odd


def fused_kernel(ring, factor, *refs):
    token_refs, weight_inputs, sum_input = refs[:3], refs[3:6], refs[6]
    outs, sum_out = refs[7:9], refs[9]
    (staged, sum_ref, whole, tok, acc, mine, near_send, near_recv, far_send, far_recv, travel,
     trade_send, trade_recv) = refs[10:23]
    (quad_ss, quad_rs, first_ss, first_rs, ring_ss, ring_rs, tok_ss, tok_rs, near_ss, near_rs,
     far_ss, far_rs, sum_ss, sum_rs, trade_ss, trade_rs, local_sem) = refs[23:]
    weight_refs = [staged.at[weight] for weight in range(3)]
    bf16, f32 = jnp.bfloat16, jnp.float32
    me = lax.axis_index("fs")
    group, lane = lax.div(me, QUAD), lax.rem(me, QUAD)
    low, high = lax.rem(lane, 2), lax.div(lane, 2)
    relative = [lane, lane + 1 - 2 * low, lane + 2 - 4 * high, QUAD - 1 - lane]
    peers = [group * QUAD + other for other in relative]
    place = ring_place(group, ring)

    def group_at(shift):
        return ring_group(lax.rem(place + shift + ring, ring), ring)

    around = [group_at(1) * QUAD + lane, group_at(-1) * QUAD + lane]
    depth = weight_refs[0].shape[0]
    width = whole.shape[2]
    chunk, half = QUAD * depth, 2 * depth
    rows = token_refs[0].shape[0]
    total_rows = tok.shape[1]
    reach = ring // 2
    per_slab = total_rows // chunk
    halves = [[high, 1 - high], [1 - high, high]]

    barrier = pltpu.get_barrier_semaphore()
    for other in peers[1:] + around:
        pl.semaphore_signal(
            barrier, inc=1, device_id={"fs": other}, device_id_type=pl.DeviceIdType.MESH
        )
    staging = [
        pltpu.make_async_copy(weight_inputs[weight], staged.at[weight], local_sem.at[6 + weight])
        for weight in range(3)
    ]
    staging.append(pltpu.make_async_copy(sum_input, sum_ref, local_sem.at[9]))
    for copy in staging:
        copy.start()
    pl.semaphore_wait(barrier, QUAD + 1)

    def remote(source, target, send, recv, other):
        return pltpu.make_async_remote_copy(
            src_ref=source,
            dst_ref=target,
            send_sem=send,
            recv_sem=recv,
            device_id={"fs": other},
            device_id_type=pl.DeviceIdType.MESH,
        )

    def slab(weight, owner, member):
        first = pl.multiple_of((owner * QUAD + member) * depth, depth)
        return whole.at[weight, pl.ds(first, depth), :]

    def columns(weight, member):
        return weight_refs[weight].at[:, pl.ds(pl.multiple_of(member * width, width), width)]

    def half_slab(weight, owner, part):
        first = pl.multiple_of(owner * chunk + part * half, half)
        return whole.at[weight, pl.ds(first, half), :]

    sent, kept = [], []

    def begin(copy):
        copy.start()
        sent.append(copy)
        return copy

    quad, first_hop, hop, tokens = {}, {}, {}, {}

    def hop_first(weight, piece):
        for way in range(2):
            target = slab(weight, group, relative[piece])
            first_hop[weight, way, piece] = begin(
                remote(
                    columns(weight, lane) if piece == 0 else target,
                    target,
                    first_ss.at[weight, way, piece],
                    first_rs.at[weight, way, piece],
                    around[way],
                )
            )

    for weight in range(3):
        staging[weight].wait()
        for far in (1, 3, 2):
            quad[weight, far] = begin(
                remote(
                    columns(weight, relative[far]),
                    slab(weight, group, lane),
                    quad_ss.at[weight, far - 1],
                    quad_rs.at[weight, far - 1],
                    peers[far],
                )
            )
        if weight < 2:
            hop_first(weight, 0)

    for weight in range(3):
        copy = pltpu.make_async_copy(
            columns(weight, lane), slab(weight, group, lane), local_sem.at[weight]
        )
        copy.start()
        kept.append(copy)

    def row_block(token, block):
        return tok.at[token, pl.ds(block * rows, rows), :]

    def send_rows(token, source, block, slot, other):
        tokens[token, slot] = begin(
            remote(
                source,
                row_block(token, block),
                tok_ss.at[token, slot],
                tok_rs.at[token, slot],
                other,
            )
        )

    for token in range(3):
        send_rows(token, token_refs[token], 2, 1, peers[2])
        send_rows(token, token_refs[token], 1, 0, peers[1])
        copy = pltpu.make_async_copy(
            token_refs[token], row_block(token, 0), local_sem.at[3 + token]
        )
        copy.start()
        kept.append(copy)

    def clear(index, carry):
        acc[index] = jnp.zeros(acc.shape[1:], f32)
        return carry

    lax.fori_loop(0, 4, clear, 0)
    acc[acc.shape[0] - 1] = jnp.zeros(acc.shape[1:], f32)

    for weight in (0, 1):
        quad[weight, 1].wait_recv()
        hop_first(weight, 1)
    hop_first(2, 0)
    quad[2, 1].wait_recv()
    hop_first(2, 1)
    for weight in range(3):
        for piece in (3, 2):
            quad[weight, piece].wait_recv()
            hop_first(weight, piece)
    for copy in kept + staging[3:]:
        copy.wait()

    arrived = set()

    def arrival(weight, way, step, order):
        if (weight, way, step, order) in arrived:
            return
        arrived.add((weight, way, step, order))
        if step == 1:
            own_half = (order == 0) == (way == 0)
            for piece in (0, 1) if own_half else (3, 2):
                first_hop[weight, way, piece].wait_recv()
        else:
            hop[weight, way, step, order].wait_recv()

    def forward(weight, step, order):
        for way in range(2):
            arrival(weight, way, step - 1, order)
            shift = (1 - step) if way == 0 else (step - 1)
            part = half_slab(weight, group_at(shift), halves[way][order])
            hop[weight, way, step, order] = begin(
                remote(
                    part,
                    part,
                    ring_ss.at[weight, way, step - 2, order],
                    ring_rs.at[weight, way, step - 2, order],
                    around[way],
                )
            )

    def arrive(weight, distance):
        for way in range(2):
            for order in range(1 if distance == reach else 2):
                arrival(weight, way, distance, order)

    def token_over(token):
        tokens[token, 1].wait_recv()
        send_rows(token, row_block(token, 2), 3, 2, peers[1])

    def token_in(token):
        tokens[token, 0].wait_recv()
        tokens[token, 2].wait_recv()

    def span(owner):
        return pl.ds(pl.multiple_of(owner * chunk, chunk), chunk)

    def project(token, shift):
        where = span(group_at(shift))
        left = tok[token, :, where]
        for weight in range(2):
            slot = 2 * token + weight
            acc[slot] += jnp.dot(left, whole[weight, where, :], preferred_element_type=f32)

    def loop(first, last, body):
        def step(index, carry):
            body(index)
            return carry

        lax.fori_loop(first, last, step, 0)

    def project_pair(distance, token_list):
        if distance == reach:
            loop(0, len(token_list), lambda i: project(token_list[0] + i, reach))
        else:
            loop(
                0,
                2 * len(token_list),
                lambda i: project(
                    token_list[0] + lax.div(i, 2), (2 * lax.rem(i, 2) - 1) * distance
                ),
            )

    for order in range(2):
        for weight in (0, 1):
            forward(weight, 2, order)
    token_over(0)
    token_in(0)
    loop(0, 3, lambda i: project(0, i - 1))
    later_started = False
    for step in range(3, reach + 1):
        last = step == reach
        if last:
            token_over(1)
            token_in(1)
            loop(0, 3, lambda i: project(1, i - 1))
            for distance in range(2, reach - 1):
                project_pair(distance, [1])
        for order in range(1 if last else 2):
            for weight in (0, 1):
                forward(weight, step, order)
        if last:
            for order in range(2):
                forward(2, 2, order)
        for weight in (0, 1):
            arrive(weight, step - 1)
        project_pair(step - 1, [0, 1] if last else [0])
    token_over(2)
    for weight in (0, 1):
        arrive(weight, reach)
    project_pair(reach, [0, 1])
    for token in range(2):
        for slot in range(3):
            tokens[token, slot].wait_send()
            sent[:] = [copy for copy in sent if copy is not tokens[token, slot]]

    tile = 32

    def early_values(index):
        where = pl.ds(pl.multiple_of(index * tile, tile), tile)
        gate, up = acc[0, where, :], acc[1, where, :]
        sig = jax.nn.sigmoid(gate)
        act = gate * sig
        tok[0, where, 0:width] = (act * up).astype(bf16)
        acc[0, where, :] = up * sig * (1.0 + gate * (1.0 - sig))
        acc[1, where, :] = act

    def later_values(index):
        where = pl.ds(pl.multiple_of(index * tile, tile), tile)
        gate, up = acc[2, where, :], acc[3, where, :]
        tok[1, where, 0:width] = (gate * jax.nn.sigmoid(gate) * up).astype(bf16)

    loop(0, total_rows // tile, early_values)
    forward(2, 3, 0)
    loop(0, total_rows // tile, later_values)
    token_in(2)

    def slab_of(index):
        if isinstance(index, int):
            return 2 + index // per_slab, index % per_slab * chunk
        first = pl.multiple_of(lax.rem(index, per_slab) * chunk, chunk)
        return 2 + lax.div(index, per_slab), first

    def partial_sum(index):
        left = tok[2, :, span(group_at(index))]
        place_of, first = slab_of(index)
        acc[place_of, pl.ds(first, chunk), :] = lax.dot_general(
            left, tok[0, :, 0:width], (((0,), (0,)), ((), ())), preferred_element_type=f32
        )

    def own_part(shift, part):
        place_of, first = slab_of((shift + ring) % ring)
        return acc[place_of, pl.ds(pl.multiple_of(first + part * half, half), half), :]

    def near_copy(which, owner):
        return remote(
            near_send.at[which, owner],
            near_recv.at[which, owner],
            near_ss.at[which, owner],
            near_rs.at[which, owner],
            peers[1],
        )

    def far_copy(which, owner):
        return remote(
            far_send.at[which, owner],
            far_recv.at[which, owner],
            far_ss.at[which, owner],
            far_rs.at[which, owner],
            peers[2],
        )

    def produce(which, owner, value):
        mine[which, owner, 0] = value[:rows]
        mine[which, owner, 1] = value[2 * rows : 3 * rows]
        near_send[which, owner, 0] = value[rows : 2 * rows].astype(bf16)
        near_send[which, owner, 1] = value[3 * rows :].astype(bf16)
        near_copy(which, owner).start()

    def relay(which, owner):
        near_copy(which, owner).wait_recv()
        mine[which, owner, 0] += near_recv[which, owner, 0].astype(f32)
        far_send[which, owner] = (
            mine[which, owner, 1] + near_recv[which, owner, 1].astype(f32)
        ).astype(bf16)
        far_copy(which, owner).start()

    def finish(which, owner):
        far_copy(which, owner).wait_recv()
        outs[which][:, span(owner)] = (
            mine[which, owner, 0] + far_recv[which, owner].astype(f32)
        ).astype(bf16)

    last_slab = acc.shape[0] - 1

    def down_step(shift):
        owner = group_at(shift)
        where = span(owner)
        right = whole[2, where, :]
        produce(0, owner, contract_last(tok[1, :, 0:width], right))
        acc[last_slab] += jnp.dot(tok[2, :, where], right, preferred_element_type=f32)

    moved = {}

    def pass_on(way, step, order, add=True):
        part = halves[way][order]
        shift = (reach + 1 - step) * (1 if way == 0 else -1)
        slot = travel.at[way, step - 1, order]
        if add:
            moved[way, step - 1, order].wait_recv()
            slot[...] = (slot[...].astype(f32) + own_part(shift, part)).astype(bf16)
        else:
            slot[...] = own_part(shift, part).astype(bf16)
        moved[way, step, order] = begin(
            remote(
                slot,
                travel.at[way, step, order],
                sum_ss.at[way, step - 1, order],
                sum_rs.at[way, step - 1, order],
                around[way],
            )
        )

    def grads(index):
        where = pl.ds(pl.multiple_of(index * tile, tile), tile)
        hidden = acc[last_slab, where, :]
        tok[0, where, width : 2 * width] = (hidden * acc[0, where, :]).astype(bf16)
        tok[1, where, width : 2 * width] = (hidden * acc[1, where, :]).astype(bf16)

    def input_step(owner):
        where = span(owner)
        produce(
            1,
            owner,
            contract_last(tok[0, :, width : 2 * width], whole[0, where, :])
            + contract_last(tok[1, :, width : 2 * width], whole[1, where, :]),
        )

        @pl.when(owner > 0)
        def _():
            relay(1, owner - 1)

    def both(distance, body):
        loop(0, 2, lambda i: body((2 * i - 1) * distance))

    def relay_at(shift):
        relay(0, group_at(shift))

    loop(0, 3, lambda i: down_step(i - 1))
    forward(2, 3, 1)
    loop(0, 3, lambda i: relay_at(i - 1))
    loop(reach - 1, reach + 2, partial_sum)
    pass_on(0, 1, 1, False)
    forward(2, reach, 0)
    pass_on(1, 1, 1, False)
    pass_on(1, 2, 0, False)
    loop(0, ring - 3, lambda i: partial_sum(lax.rem(reach + 2 + i, ring)))
    for distance in range(2, reach):
        arrive(2, distance)
        both(distance, down_step)
        both(distance, relay_at)
    pass_on(0, 2, 1)
    pass_on(0, 2, 0, False)
    arrive(2, reach)
    pass_on(1, 2, 1)
    down_step(reach)
    loop(0, total_rows // tile, grads)
    relay_at(reach)
    loop(0, ring // 2 - 1, input_step)
    pass_on(0, 3, 1)
    pass_on(1, 3, 0)
    loop(ring // 2 - 1, ring - 1, input_step)
    pass_on(0, 3, 0)
    pass_on(1, 3, 1)
    loop(ring - 1, ring, input_step)
    relay(1, ring - 1)
    loop(0, ring, lambda i: finish(0, i))
    pass_on(0, 4, 1)
    pass_on(1, 4, 0)
    loop(0, ring // 2, lambda i: finish(1, i))
    pass_on(0, 4, 0)
    pass_on(1, 4, 1)
    loop(ring // 2, ring - 2, lambda i: finish(1, i))

    def total_of(part, order_pair):
        for way in range(2):
            moved[way, reach, order_pair[way]].wait_recv()
        return (
            own_part(0, part)
            + travel[0, reach, order_pair[0]].astype(f32)
            + travel[1, reach, order_pair[1]].astype(f32)
        )

    far_pair, near_pair = (1, 0), (0, 1)

    def trade(piece, member):
        first = pl.multiple_of(member * depth, depth)
        return begin(
            remote(
                trade_send.at[pl.ds(first, depth), :],
                trade_recv.at[piece - 1],
                trade_ss.at[piece - 1],
                trade_rs.at[piece - 1],
                peers[piece],
            )
        )

    far_rows = pl.ds(pl.multiple_of((1 - high) * half, half), half)
    near_rows = pl.ds(pl.multiple_of(high * half, half), half)
    trade_send[far_rows, :] = total_of(1 - high, far_pair).astype(bf16)
    trades = {piece: trade(piece, relative[piece]) for piece in (2, 3)}
    loop(ring - 2, ring, lambda i: finish(1, i))
    own_sum = total_of(high, near_pair)
    trade_send[near_rows, :] = own_sum.astype(bf16)
    trades[1] = trade(1, relative[1])
    place_of, first = slab_of(0)
    acc[place_of, pl.ds(pl.multiple_of(first + high * half, half), half), :] = own_sum

    def across(member):
        return pl.ds(pl.multiple_of(member * width, width), width)

    own_rows = pl.ds(pl.multiple_of(first + lane * depth, depth), depth)
    sum_out[:, across(lane)] = sum_ref[:, across(lane)] + acc[place_of, own_rows, :] * factor
    for piece in (1, 2, 3):
        trades[piece].wait_recv()
        there = across(relative[piece])
        sum_out[:, there] = sum_ref[:, there] + trade_recv[piece - 1].astype(f32) * factor

    for copy in sent:
        copy.wait_send()

    def drain(index):
        which, owner = lax.div(index, ring), lax.rem(index, ring)
        near_copy(which, owner).wait_send()
        far_copy(which, owner).wait_send()

    loop(0, 2 * ring, drain)


def fused_shards(
    later_input, earlier_input, cotangent, gate_weight, up_weight, down_weight, down_grad_sum
):
    ring = lax.axis_size("fs") // QUAD
    rows, model = later_input.shape
    depth, hidden = gate_weight.shape
    width, chunk, total_rows = hidden // QUAD, QUAD * depth, QUAD * rows
    reach = ring // 2
    slabs = 2 + max(2, pl.cdiv(ring, total_rows // chunk)) + 1
    dma = pltpu.SemaphoreType.DMA
    bf16, f32 = jnp.bfloat16, jnp.float32
    vmem, anywhere = pl.BlockSpec(memory_space=pltpu.VMEM), pl.BlockSpec(memory_space=pl.ANY)
    factor = (rows * lax.axis_size("fs")) ** (-0.5)
    return tuple(
        pl.pallas_call(
            functools.partial(fused_kernel, ring, factor),
            out_shape=[
                pltpu.VMEM(later_input.shape, bf16),
                pltpu.VMEM(earlier_input.shape, bf16),
                pltpu.VMEM(down_grad_sum.shape, f32),
            ],
            in_specs=[anywhere] * 7,
            out_specs=[vmem] * 3,
            scratch_shapes=[
                pltpu.VMEM((3, depth, hidden), bf16),
                pltpu.VMEM((depth, hidden), f32),
                pltpu.VMEM((3, model, width), bf16),
                pltpu.VMEM((3, total_rows, model), bf16),
                pltpu.VMEM((slabs, total_rows, width), f32),
                pltpu.VMEM((2, ring, 2, rows, chunk), f32),
                pltpu.VMEM((2, ring, 2, rows, chunk), bf16),
                pltpu.VMEM((2, ring, 2, rows, chunk), bf16),
                pltpu.VMEM((2, ring, rows, chunk), bf16),
                pltpu.VMEM((2, ring, rows, chunk), bf16),
                pltpu.VMEM((2, reach + 1, 2, 2 * depth, width), bf16),
                pltpu.VMEM((chunk, width), bf16),
                pltpu.VMEM((3, depth, width), bf16),
                dma((3, 3)),
                dma((3, 3)),
                dma((3, 2, QUAD)),
                dma((3, 2, QUAD)),
                dma((3, 2, reach - 1, 2)),
                dma((3, 2, reach - 1, 2)),
                dma((3, 3)),
                dma((3, 3)),
                dma((2, ring)),
                dma((2, ring)),
                dma((2, ring)),
                dma((2, ring)),
                dma((2, reach, 2)),
                dma((2, reach, 2)),
                dma((3,)),
                dma((3,)),
                dma((10,)),
            ],
            compiler_params=pltpu.CompilerParams(
                collective_id=0, has_side_effects=True, vmem_limit_bytes=62_000_000
            ),
        )(
            earlier_input,
            later_input,
            cotangent,
            gate_weight,
            up_weight,
            down_weight,
            down_grad_sum,
        )
    )


def fits(mesh):
    return mesh.shape["tp"] == 1 and mesh.shape["fs"] == 8 * QUAD


def solution(mesh):
    in_specs = (
        P(("fs", "tp"), None),
        P(("fs", "tp"), None),
        P(("fs", "tp"), None),
        P("fs", "tp"),
        P("fs", "tp"),
        P("fs", "tp"),
        P("fs", "tp"),
    )
    out_specs = (P(("fs", "tp"), None), P(("fs", "tp"), None), P("fs", "tp"))
    body = fused_shards if fits(mesh) else shards
    return jax.shard_map(body, mesh=mesh, in_specs=in_specs, out_specs=out_specs, check_vma=False)
```

```python
import functools

import jax
import jax.numpy as jnp
from jax import lax
from jax.experimental import pallas as pl
from jax.experimental.pallas import tpu as pltpu
from jax.sharding import PartitionSpec as P

QUAD = 4


def contract_last(leading, trailing):
    return lax.dot_general(
        leading, trailing, (((1,), (1,)), ((), ())), preferred_element_type=jnp.float32
    )


def add_parts(received, group):
    pieces = received.reshape(group, received.shape[0] // group, received.shape[1])
    return jnp.sum(pieces.astype(jnp.float32), axis=0).astype(jnp.bfloat16)


def shards(
    later_input, earlier_input, cotangent, gate_weight, up_weight, down_weight, down_grad_sum
):
    group = lax.axis_size("tp")
    later_rows, early_rows, grad_rows = (
        lax.all_gather(later_input, "tp", axis=0, tiled=True),
        lax.all_gather(earlier_input, "tp", axis=0, tiled=True),
        lax.all_gather(cotangent, "tp", axis=0, tiled=True),
    )
    columns = later_rows
    gate_later = jnp.dot(
        columns,
        lax.all_gather(gate_weight, "fs", axis=0, tiled=True),
        preferred_element_type=jnp.float32,
    )
    up_later = jnp.dot(
        columns,
        lax.all_gather(up_weight, "fs", axis=0, tiled=True),
        preferred_element_type=jnp.float32,
    )
    hidden_later = (jax.nn.silu(gate_later) * up_later).astype(jnp.bfloat16)
    partials = contract_last(hidden_later, lax.all_gather(down_weight, "fs", axis=0, tiled=True))
    gate_whole, up_whole, down_whole = (
        lax.all_gather(gate_weight, "fs", axis=0, tiled=True),
        lax.all_gather(up_weight, "fs", axis=0, tiled=True),
        lax.all_gather(down_weight, "fs", axis=0, tiled=True),
    )
    output_received = lax.all_to_all(
        partials.astype(jnp.bfloat16), "tp", split_axis=0, concat_axis=0, tiled=True
    )
    later_output = add_parts(output_received, group)
    gate_early = jnp.dot(early_rows, gate_whole, preferred_element_type=jnp.float32)
    up_early = jnp.dot(early_rows, up_whole, preferred_element_type=jnp.float32)
    sigmoid_gate = jax.nn.sigmoid(gate_early)
    activated = gate_early * sigmoid_gate
    hidden_early = (activated * up_early).astype(jnp.bfloat16)
    grad_hidden = jnp.dot(grad_rows, down_whole, preferred_element_type=jnp.float32)
    grad_gate = (
        grad_hidden * up_early * sigmoid_gate * (1.0 + gate_early * (1.0 - sigmoid_gate))
    ).astype(jnp.bfloat16)
    grad_up = (grad_hidden * activated).astype(jnp.bfloat16)
    input_partial = contract_last(grad_gate, gate_whole) + contract_last(grad_up, up_whole)
    input_received = lax.all_to_all(
        input_partial.astype(jnp.bfloat16), "tp", split_axis=0, concat_axis=0, tiled=True
    )
    earlier_grad_input = add_parts(input_received, group)
    columns = grad_rows
    summed = lax.psum_scatter(
        lax.dot_general(
            columns, hidden_early, (((0,), (0,)), ((), ())), preferred_element_type=jnp.float32
        ),
        "fs",
        scatter_dimension=0,
        tiled=True,
    )
    factor = (later_rows.shape[0] * lax.axis_size("fs")) ** (-0.5)
    return (later_output, earlier_grad_input, down_grad_sum + summed * factor)

def ring_group(place, ring):
    half = lax.div(2 * place, ring)
    return 2 * place * (1 - half) + (2 * (ring - 1 - place) + 1) * half


def ring_place(group, ring):
    odd = lax.rem(group, 2)
    return lax.div(group, 2) * (1 - odd) + (ring - 1 - lax.div(group, 2)) * odd


def fused_kernel(ring, factor, *refs):
    token_refs, weight_inputs, sum_input = refs[:3], refs[3:6], refs[6]
    outs, sum_out = refs[7:9], refs[9]
    (staged, sum_ref, whole, tok, acc, mine, near_send, near_recv, far_send, far_recv, travel,
     trade_send, trade_recv) = refs[10:23]
    (quad_ss, quad_rs, first_rs, ring_ss, ring_rs, tok_ss, tok_rs, near_ss, near_rs,
     far_ss, far_rs, sum_ss, sum_rs, last_rs, trade_ss, trade_rs, local_sem) = refs[23:]
    weight_refs = [staged.at[weight] for weight in range(3)]
    bf16, f32 = jnp.bfloat16, jnp.float32
    me = lax.axis_index("fs")
    group, lane = lax.div(me, QUAD), lax.rem(me, QUAD)
    low, high = lax.rem(lane, 2), lax.div(lane, 2)
    relative = [lane, lane + 1 - 2 * low, lane + 2 - 4 * high, QUAD - 1 - lane]
    peers = [group * QUAD + other for other in relative]
    place = ring_place(group, ring)

    def group_at(shift):
        return ring_group(lax.rem(place + shift + ring, ring), ring)

    around = [group_at(1) * QUAD + lane, group_at(-1) * QUAD + lane]
    depth = weight_refs[0].shape[0]
    width = whole.shape[2]
    chunk, half = QUAD * depth, 2 * depth
    rows = token_refs[0].shape[0]
    total_rows = tok.shape[1]
    reach = ring // 2
    per_slab = total_rows // chunk
    halves = [[high, 1 - high], [1 - high, high]]

    barrier = pltpu.get_barrier_semaphore()
    for other in peers[1:] + around:
        pl.semaphore_signal(
            barrier, inc=1, device_id={"fs": other}, device_id_type=pl.DeviceIdType.MESH
        )
    staging = [
        pltpu.make_async_copy(weight_inputs[weight], staged.at[weight], local_sem.at[2 + weight])
        for weight in range(3)
    ]
    staging.append(pltpu.make_async_copy(sum_input, sum_ref, local_sem.at[5]))
    for copy in staging:
        copy.start()
    pl.semaphore_wait(barrier, QUAD + 1)

    def remote(source, target, send, recv, other):
        return pltpu.make_async_remote_copy(
            src_ref=source,
            dst_ref=target,
            send_sem=send,
            recv_sem=recv,
            device_id={"fs": other},
            device_id_type=pl.DeviceIdType.MESH,
        )

    def slab(weight, owner, member):
        first = pl.multiple_of((owner * QUAD + member) * depth, depth)
        return whole.at[weight, pl.ds(first, depth), :]

    def columns(weight, member):
        return weight_refs[weight].at[:, pl.ds(pl.multiple_of(member * width, width), width)]

    def half_slab(weight, owner, part):
        first = pl.multiple_of(owner * chunk + part * half, half)
        return whole.at[weight, pl.ds(first, half), :]

    def begin(copy):
        copy.start()
        return copy

    def settle(part, send):
        remote(part, part, send, send, peers[1]).wait_send()

    quad, first_hop, hop, tokens = {}, {}, {}, {}

    def hop_first(weight, piece):
        for way in range(2):
            target = slab(weight, group, relative[piece])
            first_hop[weight, way, piece] = begin(
                remote(
                    columns(weight, lane) if piece == 0 else target,
                    target,
                    ring_ss.at[weight, way],
                    first_rs.at[weight, way, 0 if piece < 2 else 1],
                    around[way],
                )
            )

    for weight in range(3):
        staging[weight].wait()
        for far in (1, 3, 2):
            quad[weight, far] = begin(
                remote(
                    columns(weight, relative[far]),
                    slab(weight, group, lane),
                    quad_ss.at[weight],
                    quad_rs.at[weight, far - 1],
                    peers[far],
                )
            )
        if weight < 2:
            hop_first(weight, 0)

    for weight in range(3):
        copy = pltpu.make_async_copy(
            columns(weight, lane), slab(weight, group, lane), local_sem.at[0]
        )
        copy.start()

    def row_block(token, block):
        return tok.at[token, pl.ds(block * rows, rows), :]

    def send_rows(token, source, block, slot, other):
        tokens[token, slot] = begin(
            remote(
                source,
                row_block(token, block),
                tok_ss.at[token],
                tok_rs.at[token, slot],
                other,
            )
        )

    for token in range(3):
        send_rows(token, token_refs[token], 2, 1, peers[2])
        send_rows(token, token_refs[token], 1, 0, peers[1])
        copy = pltpu.make_async_copy(
            token_refs[token], row_block(token, 0), local_sem.at[1]
        )
        copy.start()

    def clear(index, carry):
        acc[index] = jnp.zeros(acc.shape[1:], f32)
        return carry

    lax.fori_loop(0, 4, clear, 0)
    acc[acc.shape[0] - 1] = jnp.zeros(acc.shape[1:], f32)

    for weight in (0, 1):
        quad[weight, 1].wait_recv()
        hop_first(weight, 1)
    hop_first(2, 0)
    quad[2, 1].wait_recv()
    hop_first(2, 1)
    for weight in range(3):
        for piece in (3, 2):
            quad[weight, piece].wait_recv()
            hop_first(weight, piece)
    staging[3].wait()
    for part, index in ((whole.at[0, 0 : 3 * depth], 0), (tok.at[0, 0 : 3 * rows], 1)):
        pltpu.make_async_copy(part, part, local_sem.at[index]).wait()

    arrived = set()

    def arrival(weight, way, step, order):
        if (weight, way, step, order) in arrived:
            return
        arrived.add((weight, way, step, order))
        if step == 1:
            side = 0 if (order == 0) == (way == 0) else 1
            part = half_slab(weight, group_at(-1 if way == 0 else 1), halves[way][order])
            slot = first_rs.at[weight, way, side]
            remote(part, part, slot, slot, peers[1]).wait_recv()
        else:
            hop[weight, way, step, order].wait_recv()

    def forward(weight, step, order):
        for way in range(2):
            arrival(weight, way, step - 1, order)
            shift = (1 - step) if way == 0 else (step - 1)
            part = half_slab(weight, group_at(shift), halves[way][order])
            hop[weight, way, step, order] = begin(
                remote(
                    part,
                    part,
                    ring_ss.at[weight, way],
                    ring_rs.at[weight, way, step - 2, order],
                    around[way],
                )
            )

    def arrive(weight, distance):
        for way in range(2):
            for order in range(1 if distance == reach else 2):
                arrival(weight, way, distance, order)

    def token_over(token):
        tokens[token, 1].wait_recv()
        send_rows(token, row_block(token, 2), 3, 2, peers[1])

    def token_in(token):
        tokens[token, 0].wait_recv()
        tokens[token, 2].wait_recv()

    def span(owner):
        return pl.ds(pl.multiple_of(owner * chunk, chunk), chunk)

    def project(token, shift):
        where = span(group_at(shift))
        left = tok[token, :, where]
        for weight in range(2):
            slot = 2 * token + weight
            acc[slot] += jnp.dot(left, whole[weight, where, :], preferred_element_type=f32)

    def loop(first, last, body):
        def step(index, carry):
            body(index)
            return carry

        lax.fori_loop(first, last, step, 0)

    def project_pair(distance, token_list):
        if distance == reach:
            loop(0, len(token_list), lambda i: project(token_list[0] + i, reach))
        else:
            loop(
                0,
                2 * len(token_list),
                lambda i: project(
                    token_list[0] + lax.div(i, 2), (2 * lax.rem(i, 2) - 1) * distance
                ),
            )

    for order in range(2):
        for weight in (0, 1):
            forward(weight, 2, order)
    token_over(0)
    token_in(0)
    loop(0, 3, lambda i: project(0, i - 1))
    later_started = False
    for step in range(3, reach + 1):
        last = step == reach
        if last:
            token_over(1)
            token_in(1)
            loop(0, 3, lambda i: project(1, i - 1))
            for distance in range(2, reach - 1):
                project_pair(distance, [1])
        for order in range(1 if last else 2):
            for weight in (0, 1):
                forward(weight, step, order)
        if last:
            for order in range(2):
                forward(2, 2, order)
        for weight in (0, 1):
            arrive(weight, step - 1)
        project_pair(step - 1, [0, 1] if last else [0])
    token_over(2)
    for weight in (0, 1):
        arrive(weight, reach)
    project_pair(reach, [0, 1])
    for token in range(2):
        settle(tok.at[token, 0 : 3 * rows], tok_ss.at[token])

    tile = 32

    def early_values(index):
        where = pl.ds(pl.multiple_of(index * tile, tile), tile)
        gate, up = acc[0, where, :], acc[1, where, :]
        sig = jax.nn.sigmoid(gate)
        act = gate * sig
        tok[0, where, 0:width] = (act * up).astype(bf16)
        acc[0, where, :] = up * sig * (1.0 + gate * (1.0 - sig))
        acc[1, where, :] = act

    def later_values(index):
        where = pl.ds(pl.multiple_of(index * tile, tile), tile)
        gate, up = acc[2, where, :], acc[3, where, :]
        tok[1, where, 0:width] = (gate * jax.nn.sigmoid(gate) * up).astype(bf16)

    loop(0, total_rows // tile, early_values)
    forward(2, 3, 0)
    loop(0, total_rows // tile, later_values)
    token_in(2)

    def slab_of(index):
        if isinstance(index, int):
            return 2 + index // per_slab, index % per_slab * chunk
        first = pl.multiple_of(lax.rem(index, per_slab) * chunk, chunk)
        return 2 + lax.div(index, per_slab), first

    def partial_sum(index):
        left = tok[2, :, span(group_at(index))]
        place_of, first = slab_of(index)
        acc[place_of, pl.ds(first, chunk), :] = lax.dot_general(
            left, tok[0, :, 0:width], (((0,), (0,)), ((), ())), preferred_element_type=f32
        )

    def own_part(shift, part):
        place_of, first = slab_of((shift + ring) % ring)
        return acc[place_of, pl.ds(pl.multiple_of(first + part * half, half), half), :]

    def near_copy(which, owner):
        return remote(
            near_send.at[which, owner],
            near_recv.at[which, owner],
            near_ss.at[which],
            near_rs.at[which, owner],
            peers[1],
        )

    def far_copy(which, owner):
        return remote(
            far_send.at[which, owner],
            far_recv.at[which, owner],
            far_ss.at[which],
            far_rs.at[which, owner],
            peers[2],
        )

    def produce(which, owner, value):
        mine[which, owner, 0] = value[:rows]
        mine[which, owner, 1] = value[2 * rows : 3 * rows]
        near_send[which, owner, 0] = value[rows : 2 * rows].astype(bf16)
        near_send[which, owner, 1] = value[3 * rows :].astype(bf16)
        near_copy(which, owner).start()

    def relay(which, owner):
        near_copy(which, owner).wait_recv()
        mine[which, owner, 0] += near_recv[which, owner, 0].astype(f32)
        far_send[which, owner] = (
            mine[which, owner, 1] + near_recv[which, owner, 1].astype(f32)
        ).astype(bf16)
        far_copy(which, owner).start()

    def finish(which, owner):
        far_copy(which, owner).wait_recv()
        outs[which][:, span(owner)] = (
            mine[which, owner, 0] + far_recv[which, owner].astype(f32)
        ).astype(bf16)

    last_slab = acc.shape[0] - 1

    def down_step(shift):
        owner = group_at(shift)
        where = span(owner)
        right = whole[2, where, :]
        produce(0, owner, contract_last(tok[1, :, 0:width], right))
        acc[last_slab] += jnp.dot(tok[2, :, where], right, preferred_element_type=f32)

    moved = {}

    def pass_on(way, step, order, add=True):
        part = halves[way][order]
        shift = (reach + 1 - step) * (1 if way == 0 else -1)
        slot = travel.at[way, step - 1, order]
        if add:
            moved[way, step - 1, order].wait_recv()
            slot[...] = (slot[...].astype(f32) + own_part(shift, part)).astype(bf16)
        else:
            slot[...] = own_part(shift, part).astype(bf16)
        if step == reach and order == way:
            for index, member in enumerate((1 - low, low)):
                where = pl.ds(pl.multiple_of(member * depth, depth), depth)
                moved[way, step, order, index] = begin(
                    remote(
                        slot.at[where, :],
                        travel.at[way, step, order, where, :],
                        sum_ss.at[way],
                        last_rs.at[way, index],
                        around[way],
                    )
                )
            return
        moved[way, step, order] = begin(
            remote(
                slot,
                travel.at[way, step, order],
                sum_ss.at[way],
                sum_rs.at[way, step - 1, order],
                around[way],
            )
        )

    def grads(index):
        where = pl.ds(pl.multiple_of(index * tile, tile), tile)
        hidden = acc[last_slab, where, :]
        tok[0, where, width : 2 * width] = (hidden * acc[0, where, :]).astype(bf16)
        tok[1, where, width : 2 * width] = (hidden * acc[1, where, :]).astype(bf16)

    def input_step(owner):
        where = span(owner)
        produce(
            1,
            owner,
            contract_last(tok[0, :, width : 2 * width], whole[0, where, :])
            + contract_last(tok[1, :, width : 2 * width], whole[1, where, :]),
        )

        @pl.when(owner > 0)
        def _():
            relay(1, owner - 1)

    def both(distance, body):
        loop(0, 2, lambda i: body((2 * i - 1) * distance))

    def relay_at(shift):
        relay(0, group_at(shift))

    loop(0, 3, lambda i: down_step(i - 1))
    forward(2, 3, 1)
    loop(0, 3, lambda i: relay_at(i - 1))
    loop(reach - 1, reach + 2, partial_sum)
    pass_on(0, 1, 1, False)
    forward(2, reach, 0)
    pass_on(1, 1, 1, False)
    pass_on(1, 2, 0, False)
    loop(0, ring - 3, lambda i: partial_sum(lax.rem(reach + 2 + i, ring)))
    for distance in range(2, reach):
        arrive(2, distance)
        both(distance, down_step)
        both(distance, relay_at)
    pass_on(0, 2, 1)
    pass_on(0, 2, 0, False)
    arrive(2, reach)
    pass_on(1, 2, 1)
    down_step(reach)
    loop(0, total_rows // tile, grads)
    relay_at(reach)
    loop(0, ring // 2 - 1, input_step)
    pass_on(0, 3, 1)
    pass_on(1, 3, 0)
    loop(ring // 2 - 1, ring - 1, input_step)
    pass_on(0, 3, 0)
    pass_on(1, 3, 1)
    loop(ring - 1, ring, input_step)
    relay(1, ring - 1)
    loop(0, ring, lambda i: finish(0, i))
    pass_on(0, 4, 1)
    pass_on(1, 4, 0)
    loop(0, ring // 2, lambda i: finish(1, i))
    pass_on(0, 4, 0)
    pass_on(1, 4, 1)
    loop(ring // 2, ring - 2, lambda i: finish(1, i))

    def trade(piece, member):
        first = pl.multiple_of(member * depth, depth)
        return begin(
            remote(
                trade_send.at[pl.ds(first, depth), :],
                trade_recv.at[piece - 1],
                trade_ss.at[0],
                trade_rs.at[piece - 1],
                peers[piece],
            )
        )

    def across(member):
        return pl.ds(pl.multiple_of(member * width, width), width)

    def collect(piece):
        trades[piece].wait_recv()
        there = across(relative[piece])
        sum_out[:, there] = sum_ref[:, there] + trade_recv[piece - 1].astype(f32) * factor

    def near_total(index, member):
        where = pl.ds(pl.multiple_of(member * depth, depth), depth)
        for way in range(2):
            moved[way, reach, way, index].wait_recv()
        rows_of = pl.ds(pl.multiple_of(first + high * half + member * depth, depth), depth)
        return (
            acc[place_of, rows_of, :]
            + travel[0, reach, 0, where, :].astype(f32)
            + travel[1, reach, 1, where, :].astype(f32)
        )

    place_of, first = slab_of(0)
    moved[0, reach, 1].wait_recv()
    moved[1, reach, 0].wait_recv()
    trade_send[pl.ds(pl.multiple_of((1 - high) * half, half), half), :] = (
        own_part(0, 1 - high) + travel[0, reach, 1].astype(f32) + travel[1, reach, 0].astype(f32)
    ).astype(bf16)
    trades = {piece: trade(piece, relative[piece]) for piece in (2, 3)}
    loop(ring - 2, ring, lambda i: finish(1, i))
    trade_send[pl.ds(pl.multiple_of(relative[1] * depth, depth), depth), :] = near_total(
        0, 1 - low
    ).astype(bf16)
    trades[1] = trade(1, relative[1])
    collect(2)
    collect(3)
    sum_out[:, across(lane)] = sum_ref[:, across(lane)] + near_total(1, low) * factor
    collect(1)

    for weight in range(3):
        settle(whole.at[weight, 0 : 3 * depth], quad_ss.at[weight])
        for way in range(2):
            settle(whole.at[weight, 0 : (2 * reach - 1) * half], ring_ss.at[weight, way])
    settle(tok.at[2, 0 : 3 * rows], tok_ss.at[2])
    for index in range(2):
        settle(near_send.at[index], near_ss.at[index])
        settle(far_send.at[index], far_ss.at[index])
        settle(whole.at[0, 0 : (2 * reach - 1) * half], sum_ss.at[index])
    settle(trade_recv, trade_ss.at[0])


def deliver_kernel(*refs):
    sources, targets, done = refs[:3], refs[3:6], refs[6]
    copies = [
        pltpu.make_async_copy(source, target, done.at[index])
        for index, (source, target) in enumerate(zip(sources, targets))
    ]
    for copy in copies:
        copy.start()
    for copy in copies:
        copy.wait()


def fused_shards(
    later_input, earlier_input, cotangent, gate_weight, up_weight, down_weight, down_grad_sum
):
    ring = lax.axis_size("fs") // QUAD
    rows, model = later_input.shape
    depth, hidden = gate_weight.shape
    width, chunk, total_rows = hidden // QUAD, QUAD * depth, QUAD * rows
    reach = ring // 2
    slabs = 2 + max(2, pl.cdiv(ring, total_rows // chunk)) + 1
    dma = pltpu.SemaphoreType.DMA
    bf16, f32 = jnp.bfloat16, jnp.float32
    vmem, anywhere = pl.BlockSpec(memory_space=pltpu.VMEM), pl.BlockSpec(memory_space=pl.ANY)
    factor = (rows * lax.axis_size("fs")) ** (-0.5)
    shapes = [
        (later_input.shape, bf16),
        (earlier_input.shape, bf16),
        (down_grad_sum.shape, f32),
    ]
    results = pl.pallas_call(
            functools.partial(fused_kernel, ring, factor),
            out_shape=[pltpu.VMEM(*shape) for shape in shapes],
            in_specs=[anywhere] * 7,
            out_specs=[vmem] * 3,
            scratch_shapes=[
                pltpu.VMEM((3, depth, hidden), bf16),
                pltpu.VMEM((depth, hidden), f32),
                pltpu.VMEM((3, model, width), bf16),
                pltpu.VMEM((3, total_rows, model), bf16),
                pltpu.VMEM((slabs, total_rows, width), f32),
                pltpu.VMEM((2, ring, 2, rows, chunk), f32),
                pltpu.VMEM((2, ring, 2, rows, chunk), bf16),
                pltpu.VMEM((2, ring, 2, rows, chunk), bf16),
                pltpu.VMEM((2, ring, rows, chunk), bf16),
                pltpu.VMEM((2, ring, rows, chunk), bf16),
                pltpu.VMEM((2, reach + 1, 2, 2 * depth, width), bf16),
                pltpu.VMEM((chunk, width), bf16),
                pltpu.VMEM((3, depth, width), bf16),
                dma((3,)),
                dma((3, 3)),
                dma((3, 2, 2)),
                dma((3, 2)),
                dma((3, 2, reach - 1, 2)),
                dma((3,)),
                dma((3, 3)),
                dma((2,)),
                dma((2, ring)),
                dma((2,)),
                dma((2, ring)),
                dma((2,)),
                dma((2, reach, 2)),
                dma((2, 2)),
                dma((1,)),
                dma((3,)),
                dma((6,)),
            ],
            compiler_params=pltpu.CompilerParams(
                collective_id=0, has_side_effects=True, vmem_limit_bytes=62_000_000
            ),
        )(
            earlier_input,
            later_input,
            cotangent,
            gate_weight,
            up_weight,
            down_weight,
            down_grad_sum,
        )
    return tuple(
        pl.pallas_call(
            deliver_kernel,
            out_shape=[jax.ShapeDtypeStruct(*shape) for shape in shapes],
            in_specs=[vmem] * 3,
            out_specs=[anywhere] * 3,
            scratch_shapes=[dma((3,))],
            compiler_params=pltpu.CompilerParams(vmem_limit_bytes=1_000_000),
        )(*(pltpu.with_memory_space_constraint(value, pltpu.VMEM) for value in results))
    )


def fits(mesh):
    return mesh.shape["tp"] == 1 and mesh.shape["fs"] == 8 * QUAD


def solution(mesh):
    in_specs = (
        P(("fs", "tp"), None),
        P(("fs", "tp"), None),
        P(("fs", "tp"), None),
        P("fs", "tp"),
        P("fs", "tp"),
        P("fs", "tp"),
        P("fs", "tp"),
    )
    out_specs = (P(("fs", "tp"), None), P(("fs", "tp"), None), P("fs", "tp"))
    body = fused_shards if fits(mesh) else shards
    return jax.shard_map(body, mesh=mesh, in_specs=in_specs, out_specs=out_specs, check_vma=False)
```

```python
import functools

import jax
import jax.numpy as jnp
from jax import lax
from jax.experimental import pallas as pl
from jax.experimental.pallas import tpu as pltpu
from jax.sharding import PartitionSpec as P

QUAD = 4


def contract_last(leading, trailing):
    return lax.dot_general(
        leading, trailing, (((1,), (1,)), ((), ())), preferred_element_type=jnp.float32
    )


def add_parts(received, group):
    pieces = received.reshape(group, received.shape[0] // group, received.shape[1])
    return jnp.sum(pieces.astype(jnp.float32), axis=0).astype(jnp.bfloat16)


def shards(
    later_input, earlier_input, cotangent, gate_weight, up_weight, down_weight, down_grad_sum
):
    group = lax.axis_size("tp")
    later_rows, early_rows, grad_rows = (
        lax.all_gather(later_input, "tp", axis=0, tiled=True),
        lax.all_gather(earlier_input, "tp", axis=0, tiled=True),
        lax.all_gather(cotangent, "tp", axis=0, tiled=True),
    )
    columns = later_rows
    gate_later = jnp.dot(
        columns,
        lax.all_gather(gate_weight, "fs", axis=0, tiled=True),
        preferred_element_type=jnp.float32,
    )
    up_later = jnp.dot(
        columns,
        lax.all_gather(up_weight, "fs", axis=0, tiled=True),
        preferred_element_type=jnp.float32,
    )
    hidden_later = (jax.nn.silu(gate_later) * up_later).astype(jnp.bfloat16)
    partials = contract_last(hidden_later, lax.all_gather(down_weight, "fs", axis=0, tiled=True))
    gate_whole, up_whole, down_whole = (
        lax.all_gather(gate_weight, "fs", axis=0, tiled=True),
        lax.all_gather(up_weight, "fs", axis=0, tiled=True),
        lax.all_gather(down_weight, "fs", axis=0, tiled=True),
    )
    output_received = lax.all_to_all(
        partials.astype(jnp.bfloat16), "tp", split_axis=0, concat_axis=0, tiled=True
    )
    later_output = add_parts(output_received, group)
    gate_early = jnp.dot(early_rows, gate_whole, preferred_element_type=jnp.float32)
    up_early = jnp.dot(early_rows, up_whole, preferred_element_type=jnp.float32)
    sigmoid_gate = jax.nn.sigmoid(gate_early)
    activated = gate_early * sigmoid_gate
    hidden_early = (activated * up_early).astype(jnp.bfloat16)
    grad_hidden = jnp.dot(grad_rows, down_whole, preferred_element_type=jnp.float32)
    grad_gate = (
        grad_hidden * up_early * sigmoid_gate * (1.0 + gate_early * (1.0 - sigmoid_gate))
    ).astype(jnp.bfloat16)
    grad_up = (grad_hidden * activated).astype(jnp.bfloat16)
    input_partial = contract_last(grad_gate, gate_whole) + contract_last(grad_up, up_whole)
    input_received = lax.all_to_all(
        input_partial.astype(jnp.bfloat16), "tp", split_axis=0, concat_axis=0, tiled=True
    )
    earlier_grad_input = add_parts(input_received, group)
    columns = grad_rows
    summed = lax.psum_scatter(
        lax.dot_general(
            columns, hidden_early, (((0,), (0,)), ((), ())), preferred_element_type=jnp.float32
        ),
        "fs",
        scatter_dimension=0,
        tiled=True,
    )
    factor = (later_rows.shape[0] * lax.axis_size("fs")) ** (-0.5)
    return (later_output, earlier_grad_input, down_grad_sum + summed * factor)

def ring_group(place, ring):
    half = lax.div(2 * place, ring)
    return 2 * place * (1 - half) + (2 * (ring - 1 - place) + 1) * half


def ring_place(group, ring):
    odd = lax.rem(group, 2)
    return lax.div(group, 2) * (1 - odd) + (ring - 1 - lax.div(group, 2)) * odd


def fused_kernel(ring, factor, *refs):
    token_refs, weight_inputs, sum_input = refs[:3], refs[3:6], refs[6]
    outs, sum_out = refs[7:9], refs[9]
    (staged, sum_ref, whole, tok, acc, mine, near_send, near_recv, far_send, far_recv, travel,
     trade_send, trade_recv) = refs[10:23]
    (quad_ss, quad_rs, first_rs, ring_ss, ring_rs, tok_ss, tok_rs, near_ss, near_rs,
     far_ss, far_rs, sum_ss, sum_rs, trade_ss, trade_rs, local_sem) = refs[23:]
    weight_refs = [staged.at[weight] for weight in range(3)]
    bf16, f32 = jnp.bfloat16, jnp.float32
    me = lax.axis_index("fs")
    group, lane = lax.div(me, QUAD), lax.rem(me, QUAD)
    low, high = lax.rem(lane, 2), lax.div(lane, 2)
    relative = [lane, lane + 1 - 2 * low, lane + 2 - 4 * high, QUAD - 1 - lane]
    peers = [group * QUAD + other for other in relative]
    place = ring_place(group, ring)

    def group_at(shift):
        return ring_group(lax.rem(place + shift + ring, ring), ring)

    around = [group_at(1) * QUAD + lane, group_at(-1) * QUAD + lane]
    depth = weight_refs[0].shape[0]
    width = whole.shape[2]
    chunk, half = QUAD * depth, 2 * depth
    rows = token_refs[0].shape[0]
    total_rows = tok.shape[1]
    reach = ring // 2
    per_slab = total_rows // chunk
    halves = [[high, 1 - high], [1 - high, high]]

    barrier = pltpu.get_barrier_semaphore()
    for other in peers[1:] + around:
        pl.semaphore_signal(
            barrier, inc=1, device_id={"fs": other}, device_id_type=pl.DeviceIdType.MESH
        )
    staging = [
        pltpu.make_async_copy(weight_inputs[weight], staged.at[weight], local_sem.at[2 + weight])
        for weight in range(3)
    ]
    staging.append(pltpu.make_async_copy(sum_input, sum_ref, local_sem.at[5]))
    for copy in staging:
        copy.start()
    pl.semaphore_wait(barrier, QUAD + 1)

    def remote(source, target, send, recv, other):
        return pltpu.make_async_remote_copy(
            src_ref=source,
            dst_ref=target,
            send_sem=send,
            recv_sem=recv,
            device_id={"fs": other},
            device_id_type=pl.DeviceIdType.MESH,
        )

    def slab(weight, owner, member):
        first = pl.multiple_of((owner * QUAD + member) * depth, depth)
        return whole.at[weight, pl.ds(first, depth), :]

    def columns(weight, member):
        return weight_refs[weight].at[:, pl.ds(pl.multiple_of(member * width, width), width)]

    def half_slab(weight, owner, part):
        first = pl.multiple_of(owner * chunk + part * half, half)
        return whole.at[weight, pl.ds(first, half), :]

    def begin(copy):
        copy.start()
        return copy

    def settle(part, send):
        remote(part, part, send, send, peers[1]).wait_send()

    quad, first_hop, hop, tokens = {}, {}, {}, {}

    def hop_first(weight, piece):
        for way in range(2):
            target = slab(weight, group, relative[piece])
            first_hop[weight, way, piece] = begin(
                remote(
                    columns(weight, lane) if piece == 0 else target,
                    target,
                    ring_ss.at[weight, way],
                    first_rs.at[weight, way, 0 if piece < 2 else 1],
                    around[way],
                )
            )

    for weight in range(3):
        staging[weight].wait()
        for far in (1, 3, 2):
            quad[weight, far] = begin(
                remote(
                    columns(weight, relative[far]),
                    slab(weight, group, lane),
                    quad_ss.at[weight],
                    quad_rs.at[weight, far - 1],
                    peers[far],
                )
            )
        if weight < 2:
            hop_first(weight, 0)

    for weight in range(3):
        copy = pltpu.make_async_copy(
            columns(weight, lane), slab(weight, group, lane), local_sem.at[0]
        )
        copy.start()

    def row_block(token, block):
        return tok.at[token, pl.ds(block * rows, rows), :]

    def send_rows(token, source, block, slot, other):
        tokens[token, slot] = begin(
            remote(
                source,
                row_block(token, block),
                tok_ss.at[token],
                tok_rs.at[token, slot],
                other,
            )
        )

    for token in range(3):
        send_rows(token, token_refs[token], 2, 1, peers[2])
        send_rows(token, token_refs[token], 1, 0, peers[1])
        copy = pltpu.make_async_copy(
            token_refs[token], row_block(token, 0), local_sem.at[1]
        )
        copy.start()

    def clear(index, carry):
        acc[index] = jnp.zeros(acc.shape[1:], f32)
        return carry

    lax.fori_loop(0, 4, clear, 0)
    acc[acc.shape[0] - 1] = jnp.zeros(acc.shape[1:], f32)

    for weight in (0, 1):
        quad[weight, 1].wait_recv()
        hop_first(weight, 1)
    hop_first(2, 0)
    quad[2, 1].wait_recv()
    hop_first(2, 1)
    for weight in range(3):
        for piece in (3, 2):
            quad[weight, piece].wait_recv()
            hop_first(weight, piece)
    staging[3].wait()
    for part, index in ((whole.at[0, 0 : 3 * depth], 0), (tok.at[0, 0 : 3 * rows], 1)):
        pltpu.make_async_copy(part, part, local_sem.at[index]).wait()

    arrived = set()

    def arrival(weight, way, step, order):
        if (weight, way, step, order) in arrived:
            return
        arrived.add((weight, way, step, order))
        if step == 1:
            side = 0 if (order == 0) == (way == 0) else 1
            part = half_slab(weight, group_at(-1 if way == 0 else 1), halves[way][order])
            slot = first_rs.at[weight, way, side]
            remote(part, part, slot, slot, peers[1]).wait_recv()
        else:
            hop[weight, way, step, order].wait_recv()

    def forward(weight, step, order):
        for way in range(2):
            arrival(weight, way, step - 1, order)
            shift = (1 - step) if way == 0 else (step - 1)
            part = half_slab(weight, group_at(shift), halves[way][order])
            hop[weight, way, step, order] = begin(
                remote(
                    part,
                    part,
                    ring_ss.at[weight, way],
                    ring_rs.at[weight, way, step - 2, order],
                    around[way],
                )
            )

    def arrive(weight, distance):
        for way in range(2):
            for order in range(1 if distance == reach else 2):
                arrival(weight, way, distance, order)

    def token_over(token):
        tokens[token, 1].wait_recv()
        send_rows(token, row_block(token, 2), 3, 2, peers[1])

    def token_in(token):
        tokens[token, 0].wait_recv()
        tokens[token, 2].wait_recv()

    def span(owner):
        return pl.ds(pl.multiple_of(owner * chunk, chunk), chunk)

    def project(token, shift):
        where = span(group_at(shift))
        left = tok[token, :, where]
        for weight in range(2):
            slot = 2 * token + weight
            acc[slot] += jnp.dot(left, whole[weight, where, :], preferred_element_type=f32)

    def loop(first, last, body):
        def step(index, carry):
            body(index)
            return carry

        lax.fori_loop(first, last, step, 0)

    def project_pair(distance, token_list):
        if distance == reach:
            loop(0, len(token_list), lambda i: project(token_list[0] + i, reach))
        else:
            loop(
                0,
                2 * len(token_list),
                lambda i: project(
                    token_list[0] + lax.div(i, 2), (2 * lax.rem(i, 2) - 1) * distance
                ),
            )

    for order in range(2):
        for weight in (0, 1):
            forward(weight, 2, order)
    token_over(0)
    token_in(0)
    loop(0, 3, lambda i: project(0, i - 1))
    later_started = False
    for step in range(3, reach + 1):
        last = step == reach
        if last:
            token_over(1)
            token_in(1)
            loop(0, 3, lambda i: project(1, i - 1))
            for distance in range(2, reach - 1):
                project_pair(distance, [1])
        for order in range(1 if last else 2):
            for weight in (0, 1):
                forward(weight, step, order)
        if last:
            for order in range(2):
                forward(2, 2, order)
        for weight in (0, 1):
            arrive(weight, step - 1)
        project_pair(step - 1, [0, 1] if last else [0])
    token_over(2)
    for weight in (0, 1):
        arrive(weight, reach)
    project_pair(reach, [0, 1])
    for token in range(2):
        settle(tok.at[token, 0 : 3 * rows], tok_ss.at[token])

    tile = 32

    def early_values(index):
        where = pl.ds(pl.multiple_of(index * tile, tile), tile)
        gate, up = acc[0, where, :], acc[1, where, :]
        sig = jax.nn.sigmoid(gate)
        act = gate * sig
        tok[0, where, 0:width] = (act * up).astype(bf16)
        acc[0, where, :] = up * sig * (1.0 + gate * (1.0 - sig))
        acc[1, where, :] = act

    def later_values(index):
        where = pl.ds(pl.multiple_of(index * tile, tile), tile)
        gate, up = acc[2, where, :], acc[3, where, :]
        tok[1, where, 0:width] = (gate * jax.nn.sigmoid(gate) * up).astype(bf16)

    loop(0, total_rows // tile, later_values)

    def slab_of(index):
        if isinstance(index, int):
            return 2 + index // per_slab, index % per_slab * chunk
        first = pl.multiple_of(lax.rem(index, per_slab) * chunk, chunk)
        return 2 + lax.div(index, per_slab), first

    def partial_sum(index):
        left = tok[2, :, span(group_at(index))]
        place_of, first = slab_of(index)
        acc[place_of, pl.ds(first, chunk), :] = lax.dot_general(
            left, tok[0, :, 0:width], (((0,), (0,)), ((), ())), preferred_element_type=f32
        )

    def own_part(shift, part):
        place_of, first = slab_of((shift + ring) % ring)
        return acc[place_of, pl.ds(pl.multiple_of(first + part * half, half), half), :]

    def near_copy(which, owner):
        return remote(
            near_send.at[which, owner],
            near_recv.at[which, owner],
            near_ss.at[which],
            near_rs.at[which, owner],
            peers[1],
        )

    def far_copy(which, owner):
        return remote(
            far_send.at[which, owner],
            far_recv.at[which, owner],
            far_ss.at[which],
            far_rs.at[which, owner],
            peers[2],
        )

    def produce(which, owner, value):
        mine[which, owner, 0] = value[:rows]
        mine[which, owner, 1] = value[2 * rows : 3 * rows]
        near_send[which, owner, 0] = value[rows : 2 * rows].astype(bf16)
        near_send[which, owner, 1] = value[3 * rows :].astype(bf16)
        near_copy(which, owner).start()

    def relay(which, owner):
        near_copy(which, owner).wait_recv()
        mine[which, owner, 0] += near_recv[which, owner, 0].astype(f32)
        far_send[which, owner] = (
            mine[which, owner, 1] + near_recv[which, owner, 1].astype(f32)
        ).astype(bf16)
        far_copy(which, owner).start()

    def finish(which, owner):
        far_copy(which, owner).wait_recv()
        outs[which][:, span(owner)] = (
            mine[which, owner, 0] + far_recv[which, owner].astype(f32)
        ).astype(bf16)

    last_slab = acc.shape[0] - 1

    def output_step(shift):
        owner = group_at(shift)
        produce(0, owner, contract_last(tok[1, :, 0:width], whole[2, span(owner), :]))

    def hidden_step(shift):
        where = span(group_at(shift))
        acc[last_slab] += jnp.dot(
            tok[2, :, where], whole[2, where, :], preferred_element_type=f32
        )

    moved = {}

    def piece_rows(piece):
        return pl.ds(pl.multiple_of((low if piece else 1 - low) * depth, depth), depth)

    def fold(way, step, order, add=True, piece=None):
        part = halves[way][order]
        shift = (reach + 1 - step) * (1 if way == 0 else -1)
        where = slice(None) if piece is None else piece_rows(piece)
        slot = travel.at[way, step - 1, order, where, :]
        if piece is None:
            mine_part = own_part(shift, part)
        else:
            place_of, first = slab_of((shift + ring) % ring)
            member = low if piece else 1 - low
            first = pl.multiple_of(first + part * half + member * depth, depth)
            mine_part = acc[place_of, pl.ds(first, depth), :]
        if add:
            copies = moved[way, step - 1, order]
            for copy in copies if piece is None else copies[piece : piece + 1]:
                copy.wait_recv()
            slot[...] = (slot[...].astype(f32) + mine_part).astype(bf16)
        else:
            slot[...] = mine_part.astype(bf16)

    def pass_on(way, step, order, pieces=(None,)):
        for piece in pieces:
            where = slice(None) if piece is None else piece_rows(piece)
            moved.setdefault((way, step, order), []).append(
                begin(
                    remote(
                        travel.at[way, step - 1, order, where, :],
                        travel.at[way, step, order, where, :],
                        sum_ss.at[way],
                        sum_rs.at[way, step - 1, order, piece or 0],
                        around[way],
                    )
                )
            )

    def grads(index):
        where = pl.ds(pl.multiple_of(index * tile, tile), tile)
        hidden = acc[last_slab, where, :]
        tok[0, where, width : 2 * width] = (hidden * acc[0, where, :]).astype(bf16)
        tok[1, where, width : 2 * width] = (hidden * acc[1, where, :]).astype(bf16)

    def input_step(owner):
        where = span(owner)
        produce(
            1,
            owner,
            contract_last(tok[0, :, width : 2 * width], whole[0, where, :])
            + contract_last(tok[1, :, width : 2 * width], whole[1, where, :]),
        )

        @pl.when(owner > 0)
        def _():
            relay(1, owner - 1)

    def both(distance, body):
        loop(0, 2, lambda i: body((2 * i - 1) * distance))

    def relay_at(shift):
        relay(0, group_at(shift))

    def output_near(index):
        output_step(index - 1)

        @pl.when(index > 0)
        def _():
            relay_at(index - 2)

    def output_pair(distance):
        both(distance, output_step)
        both(distance, relay_at)

    loop(0, 3, output_near)
    forward(2, 3, 0)
    loop(0, total_rows // tile, early_values)
    relay_at(1)
    token_in(2)
    loop(reach - 1, reach + 2, partial_sum)
    loop(0, 2, lambda i: hidden_step(i - 1))
    forward(2, 3, 1)
    arrive(2, 2)
    output_pair(2)
    forward(2, reach, 0)
    for way in range(2):
        fold(way, 1, 1, False)
        pass_on(way, 1, 1, (None,) if way else (0, 1))
        fold(way, 2, 0, False)
        pass_on(way, 2, 0, (None,) if way else (0,))

    def step_piece(step, order, piece):
        fold(0, step, order, True, piece)
        pass_on(0, step, order, (piece,))

    hidden_step(1)
    both(2, hidden_step)
    loop(0, ring - 3, lambda i: partial_sum(lax.rem(reach + 2 + i, ring)))
    arrive(2, reach - 1)
    output_pair(reach - 1)
    both(reach - 1, hidden_step)
    arrive(2, reach)
    output_step(reach)
    hidden_step(reach)
    loop(0, total_rows // tile, grads)
    step_piece(2, 1, 0)
    relay_at(reach)
    loop(0, ring // 4, input_step)
    step_piece(2, 1, 1)
    pass_on(0, 2, 0, (1,))
    fold(1, 2, 1)
    pass_on(1, 2, 1)
    loop(ring // 4, ring - 2, input_step)
    step_piece(3, 1, 0)
    fold(1, 3, 0)
    pass_on(1, 3, 0)
    loop(ring - 2, ring, input_step)
    step_piece(3, 1, 1)
    step_piece(3, 0, 0)
    relay(1, ring - 1)
    loop(0, ring, lambda i: finish(0, i))
    step_piece(3, 0, 1)
    fold(1, 3, 1)
    pass_on(1, 3, 1)
    loop(0, ring // 2, lambda i: finish(1, i))
    step_piece(4, 1, 0)
    step_piece(4, 1, 1)
    fold(1, 4, 0)
    pass_on(1, 4, 0, (0, 1))
    loop(ring // 2, ring // 2 + 1, lambda i: finish(1, i))
    step_piece(4, 0, 0)
    step_piece(4, 0, 1)
    fold(1, 4, 1)
    pass_on(1, 4, 1, (0, 1))
    loop(ring // 2 + 1, ring - 1, lambda i: finish(1, i))

    def trade(piece, member):
        first = pl.multiple_of(member * depth, depth)
        return begin(
            remote(
                trade_send.at[pl.ds(first, depth), :],
                trade_recv.at[piece - 1],
                trade_ss.at[0],
                trade_rs.at[piece - 1],
                peers[piece],
            )
        )

    def across(member):
        return pl.ds(pl.multiple_of(member * width, width), width)

    def collect(piece):
        trades[piece].wait_recv()
        there = across(relative[piece])
        sum_out[:, there] = sum_ref[:, there] + trade_recv[piece - 1].astype(f32) * factor

    place_of, first = slab_of(0)

    def total(part, orders, piece):
        where = piece_rows(piece)
        member = low if piece else 1 - low
        mine_rows = pl.ds(pl.multiple_of(first + part * half + member * depth, depth), depth)
        result = acc[place_of, mine_rows, :]
        for way in range(2):
            moved[way, reach, orders[way]][piece].wait_recv()
            result = result + travel[way, reach, orders[way], where, :].astype(f32)
        return result

    trades = {}

    def give(piece, part, orders, index):
        first_row = pl.multiple_of(relative[piece] * depth, depth)
        trade_send[pl.ds(first_row, depth), :] = total(part, orders, index).astype(bf16)
        trades[piece] = trade(piece, relative[piece])

    give(3, 1 - high, (1, 0), 0)
    loop(ring - 1, ring, lambda i: finish(1, i))
    give(2, 1 - high, (1, 0), 1)
    give(1, high, (0, 1), 0)
    collect(3)
    sum_out[:, across(lane)] = sum_ref[:, across(lane)] + total(high, (0, 1), 1) * factor
    collect(2)
    collect(1)

    for weight in range(3):
        settle(whole.at[weight, 0 : 3 * depth], quad_ss.at[weight])
        for way in range(2):
            settle(whole.at[weight, 0 : (2 * reach - 1) * half], ring_ss.at[weight, way])
    settle(tok.at[2, 0 : 3 * rows], tok_ss.at[2])
    for index in range(2):
        settle(near_send.at[index], near_ss.at[index])
        settle(far_send.at[index], far_ss.at[index])
        settle(whole.at[0, 0 : (2 * reach - 1) * half], sum_ss.at[index])
    settle(trade_recv, trade_ss.at[0])


def deliver_kernel(*refs):
    sources, targets, done = refs[:3], refs[3:6], refs[6]
    copies = [
        pltpu.make_async_copy(source, target, done.at[index])
        for index, (source, target) in enumerate(zip(sources, targets))
    ]
    for copy in copies:
        copy.start()
    for copy in copies:
        copy.wait()


def fused_shards(
    later_input, earlier_input, cotangent, gate_weight, up_weight, down_weight, down_grad_sum
):
    ring = lax.axis_size("fs") // QUAD
    rows, model = later_input.shape
    depth, hidden = gate_weight.shape
    width, chunk, total_rows = hidden // QUAD, QUAD * depth, QUAD * rows
    reach = ring // 2
    slabs = 2 + max(2, pl.cdiv(ring, total_rows // chunk)) + 1
    dma = pltpu.SemaphoreType.DMA
    bf16, f32 = jnp.bfloat16, jnp.float32
    vmem, anywhere = pl.BlockSpec(memory_space=pltpu.VMEM), pl.BlockSpec(memory_space=pl.ANY)
    factor = (rows * lax.axis_size("fs")) ** (-0.5)
    shapes = [
        (later_input.shape, bf16),
        (earlier_input.shape, bf16),
        (down_grad_sum.shape, f32),
    ]
    results = pl.pallas_call(
            functools.partial(fused_kernel, ring, factor),
            out_shape=[pltpu.VMEM(*shape) for shape in shapes],
            in_specs=[anywhere] * 7,
            out_specs=[vmem] * 3,
            scratch_shapes=[
                pltpu.VMEM((3, depth, hidden), bf16),
                pltpu.VMEM((depth, hidden), f32),
                pltpu.VMEM((3, model, width), bf16),
                pltpu.VMEM((3, total_rows, model), bf16),
                pltpu.VMEM((slabs, total_rows, width), f32),
                pltpu.VMEM((2, ring, 2, rows, chunk), f32),
                pltpu.VMEM((2, ring, 2, rows, chunk), bf16),
                pltpu.VMEM((2, ring, 2, rows, chunk), bf16),
                pltpu.VMEM((2, ring, rows, chunk), bf16),
                pltpu.VMEM((2, ring, rows, chunk), bf16),
                pltpu.VMEM((2, reach + 1, 2, 2 * depth, width), bf16),
                pltpu.VMEM((chunk, width), bf16),
                pltpu.VMEM((3, depth, width), bf16),
                dma((3,)),
                dma((3, 3)),
                dma((3, 2, 2)),
                dma((3, 2)),
                dma((3, 2, reach - 1, 2)),
                dma((3,)),
                dma((3, 3)),
                dma((2,)),
                dma((2, ring)),
                dma((2,)),
                dma((2, ring)),
                dma((2,)),
                dma((2, reach, 2, 2)),
                dma((1,)),
                dma((3,)),
                dma((6,)),
            ],
            compiler_params=pltpu.CompilerParams(
                collective_id=0, has_side_effects=True, vmem_limit_bytes=62_000_000
            ),
        )(
            earlier_input,
            later_input,
            cotangent,
            gate_weight,
            up_weight,
            down_weight,
            down_grad_sum,
        )
    return tuple(
        pl.pallas_call(
            deliver_kernel,
            out_shape=[jax.ShapeDtypeStruct(*shape) for shape in shapes],
            in_specs=[vmem] * 3,
            out_specs=[anywhere] * 3,
            scratch_shapes=[dma((3,))],
            compiler_params=pltpu.CompilerParams(vmem_limit_bytes=1_000_000),
        )(*(pltpu.with_memory_space_constraint(value, pltpu.VMEM) for value in results))
    )


def fits(mesh):
    return mesh.shape["tp"] == 1 and mesh.shape["fs"] == 8 * QUAD


def solution(mesh):
    in_specs = (
        P(("fs", "tp"), None),
        P(("fs", "tp"), None),
        P(("fs", "tp"), None),
        P("fs", "tp"),
        P("fs", "tp"),
        P("fs", "tp"),
        P("fs", "tp"),
    )
    out_specs = (P(("fs", "tp"), None), P(("fs", "tp"), None), P("fs", "tp"))
    body = fused_shards if fits(mesh) else shards
    return jax.shard_map(body, mesh=mesh, in_specs=in_specs, out_specs=out_specs, check_vma=False)
```

```python
import functools

import jax
import jax.numpy as jnp
from jax import lax
from jax.experimental import pallas as pl
from jax.experimental.pallas import tpu as pltpu
from jax.sharding import PartitionSpec as P

QUAD = 4
PIECES = 1


def contract_last(leading, trailing):
    return lax.dot_general(
        leading, trailing, (((1,), (1,)), ((), ())), preferred_element_type=jnp.float32
    )


def add_parts(received, group):
    pieces = received.reshape(group, received.shape[0] // group, received.shape[1])
    return jnp.sum(pieces.astype(jnp.float32), axis=0).astype(jnp.bfloat16)


def shards(
    later_input, earlier_input, cotangent, gate_weight, up_weight, down_weight, down_grad_sum
):
    group = lax.axis_size("tp")
    later_rows, early_rows, grad_rows = (
        lax.all_gather(later_input, "tp", axis=0, tiled=True),
        lax.all_gather(earlier_input, "tp", axis=0, tiled=True),
        lax.all_gather(cotangent, "tp", axis=0, tiled=True),
    )
    columns = later_rows
    gate_later = jnp.dot(
        columns,
        lax.all_gather(gate_weight, "fs", axis=0, tiled=True),
        preferred_element_type=jnp.float32,
    )
    up_later = jnp.dot(
        columns,
        lax.all_gather(up_weight, "fs", axis=0, tiled=True),
        preferred_element_type=jnp.float32,
    )
    hidden_later = (jax.nn.silu(gate_later) * up_later).astype(jnp.bfloat16)
    partials = contract_last(hidden_later, lax.all_gather(down_weight, "fs", axis=0, tiled=True))
    gate_whole, up_whole, down_whole = (
        lax.all_gather(gate_weight, "fs", axis=0, tiled=True),
        lax.all_gather(up_weight, "fs", axis=0, tiled=True),
        lax.all_gather(down_weight, "fs", axis=0, tiled=True),
    )
    output_received = lax.all_to_all(
        partials.astype(jnp.bfloat16), "tp", split_axis=0, concat_axis=0, tiled=True
    )
    later_output = add_parts(output_received, group)
    gate_early = jnp.dot(early_rows, gate_whole, preferred_element_type=jnp.float32)
    up_early = jnp.dot(early_rows, up_whole, preferred_element_type=jnp.float32)
    sigmoid_gate = jax.nn.sigmoid(gate_early)
    activated = gate_early * sigmoid_gate
    hidden_early = (activated * up_early).astype(jnp.bfloat16)
    grad_hidden = jnp.dot(grad_rows, down_whole, preferred_element_type=jnp.float32)
    grad_gate = (
        grad_hidden * up_early * sigmoid_gate * (1.0 + gate_early * (1.0 - sigmoid_gate))
    ).astype(jnp.bfloat16)
    grad_up = (grad_hidden * activated).astype(jnp.bfloat16)
    input_partial = contract_last(grad_gate, gate_whole) + contract_last(grad_up, up_whole)
    input_received = lax.all_to_all(
        input_partial.astype(jnp.bfloat16), "tp", split_axis=0, concat_axis=0, tiled=True
    )
    earlier_grad_input = add_parts(input_received, group)
    columns = grad_rows
    summed = lax.psum_scatter(
        lax.dot_general(
            columns, hidden_early, (((0,), (0,)), ((), ())), preferred_element_type=jnp.float32
        ),
        "fs",
        scatter_dimension=0,
        tiled=True,
    )
    factor = (later_rows.shape[0] * lax.axis_size("fs")) ** (-0.5)
    return (later_output, earlier_grad_input, down_grad_sum + summed * factor)

def ring_group(place, ring):
    half = lax.div(2 * place, ring)
    return 2 * place * (1 - half) + (2 * (ring - 1 - place) + 1) * half


def ring_place(group, ring):
    odd = lax.rem(group, 2)
    return lax.div(group, 2) * (1 - odd) + (ring - 1 - lax.div(group, 2)) * odd


def fused_kernel(ring, factor, *refs):
    token_refs, weight_inputs, sum_input = refs[:3], refs[3:6], refs[6]
    outs, sum_out = refs[7:9], refs[9]
    (staged, sum_ref, whole, tok, acc, mine, near_send, near_recv, far_send, far_recv, travel,
     trade_send, trade_recv) = refs[10:23]
    (quad_ss, quad_rs, first_rs, ring_ss, ring_rs, tok_ss, tok_rs, near_ss, near_rs,
     far_ss, far_rs, sum_ss, sum_rs, trade_ss, trade_rs, local_sem) = refs[23:]
    weight_refs = [staged.at[weight] for weight in range(3)]
    bf16, f32 = jnp.bfloat16, jnp.float32
    me = lax.axis_index("fs")
    group, lane = lax.div(me, QUAD), lax.rem(me, QUAD)
    low, high = lax.rem(lane, 2), lax.div(lane, 2)
    relative = [lane, lane + 1 - 2 * low, lane + 2 - 4 * high, QUAD - 1 - lane]
    peers = [group * QUAD + other for other in relative]
    place = ring_place(group, ring)

    def group_at(shift):
        return ring_group(lax.rem(place + shift + ring, ring), ring)

    around = [group_at(1) * QUAD + lane, group_at(-1) * QUAD + lane]
    depth = weight_refs[0].shape[0]
    width = whole.shape[2]
    chunk, half = QUAD * depth, 2 * depth
    rows = token_refs[0].shape[0]
    total_rows = tok.shape[1]
    reach = ring // 2
    per_slab = total_rows // chunk
    halves = [[high, 1 - high], [1 - high, high]]

    barrier = pltpu.get_barrier_semaphore()
    for other in peers[1:] + around:
        pl.semaphore_signal(
            barrier, inc=1, device_id={"fs": other}, device_id_type=pl.DeviceIdType.MESH
        )
    staging = [
        pltpu.make_async_copy(weight_inputs[weight], staged.at[weight], local_sem.at[2 + weight])
        for weight in range(3)
    ]
    staging.append(pltpu.make_async_copy(sum_input, sum_ref, local_sem.at[5]))
    for copy in staging:
        copy.start()
    pl.semaphore_wait(barrier, QUAD + 1)

    def remote(source, target, send, recv, other):
        return pltpu.make_async_remote_copy(
            src_ref=source,
            dst_ref=target,
            send_sem=send,
            recv_sem=recv,
            device_id={"fs": other},
            device_id_type=pl.DeviceIdType.MESH,
        )

    def slab(weight, owner, member):
        first = pl.multiple_of((owner * QUAD + member) * depth, depth)
        return whole.at[weight, pl.ds(first, depth), :]

    def columns(weight, member):
        return weight_refs[weight].at[:, pl.ds(pl.multiple_of(member * width, width), width)]

    def half_slab(weight, owner, part):
        first = pl.multiple_of(owner * chunk + part * half, half)
        return whole.at[weight, pl.ds(first, half), :]

    def begin(copy):
        copy.start()
        return copy

    def settle(part, send):
        remote(part, part, send, send, peers[1]).wait_send()

    quad, first_hop, hop, tokens = {}, {}, {}, {}

    def hop_first(weight, piece):
        for way in range(2):
            target = slab(weight, group, relative[piece])
            first_hop[weight, way, piece] = begin(
                remote(
                    columns(weight, lane) if piece == 0 else target,
                    target,
                    ring_ss.at[weight],
                    first_rs.at[weight, way, 0 if piece < 2 else 1],
                    around[way],
                )
            )

    for weight in range(3):
        staging[weight].wait()
        for far in (1, 3, 2):
            quad[weight, far] = begin(
                remote(
                    columns(weight, relative[far]),
                    slab(weight, group, lane),
                    quad_ss.at[0],
                    quad_rs.at[weight, far - 1],
                    peers[far],
                )
            )
        if weight < 2:
            hop_first(weight, 0)

    for weight in range(3):
        copy = pltpu.make_async_copy(
            columns(weight, lane), slab(weight, group, lane), local_sem.at[0]
        )
        copy.start()

    def row_block(token, block):
        return tok.at[token, pl.ds(block * rows, rows), :]

    def send_rows(token, source, block, slot, other):
        tokens[token, slot] = begin(
            remote(
                source,
                row_block(token, block),
                tok_ss.at[token],
                tok_rs.at[token, slot % 2],
                other,
            )
        )

    for token in range(3):
        send_rows(token, token_refs[token], 2, 1, peers[2])
        send_rows(token, token_refs[token], 1, 0, peers[1])
        copy = pltpu.make_async_copy(
            token_refs[token], row_block(token, 0), local_sem.at[1]
        )
        copy.start()

    def clear(index, carry):
        acc[index] = jnp.zeros(acc.shape[1:], f32)
        return carry

    lax.fori_loop(0, 4, clear, 0)
    acc[acc.shape[0] - 1] = jnp.zeros(acc.shape[1:], f32)

    for weight in (0, 1):
        quad[weight, 1].wait_recv()
        hop_first(weight, 1)
    hop_first(2, 0)
    quad[2, 1].wait_recv()
    hop_first(2, 1)
    for weight in range(3):
        for piece in (3, 2):
            quad[weight, piece].wait_recv()
            hop_first(weight, piece)
    staging[3].wait()
    for part, index in ((whole.at[0, 0 : 3 * depth], 0), (tok.at[0, 0 : 3 * rows], 1)):
        pltpu.make_async_copy(part, part, local_sem.at[index]).wait()

    arrived = set()

    def arrival(weight, way, step, order):
        if step > 1 and weight == 0:
            weight = 1
        if (weight, way, step, order) in arrived:
            return
        arrived.add((weight, way, step, order))
        if step == 1:
            side = 0 if (order == 0) == (way == 0) else 1
            part = half_slab(weight, group_at(-1 if way == 0 else 1), halves[way][order])
            slot = first_rs.at[weight, way, side]
            remote(part, part, slot, slot, peers[1]).wait_recv()
        else:
            part = whole.at[0, 0 : half if weight == 2 else chunk]
            slot = ring_rs.at[weight - 1, way, step - 2, order]
            remote(part, part, slot, slot, peers[1]).wait_recv()

    def forward(weight, step, order):
        for way in range(2):
            arrival(weight, way, step - 1, order)
            shift = (1 - step) if way == 0 else (step - 1)
            part = half_slab(weight, group_at(shift), halves[way][order])
            hop[weight, way, step, order] = begin(
                remote(
                    part,
                    part,
                    ring_ss.at[weight],
                    ring_rs.at[max(weight - 1, 0), way, step - 2, order],
                    around[way],
                )
            )

    def arrive(weight, distance):
        for way in range(2):
            for order in range(1 if distance == reach else 2):
                arrival(weight, way, distance, order)

    def token_over(token):
        tokens[token, 1].wait_recv()
        send_rows(token, row_block(token, 2), 3, 2, peers[1])

    def token_in(token):
        part, slot = tok.at[0, 0 : 2 * rows], tok_rs.at[token, 0]
        remote(part, part, slot, slot, peers[1]).wait_recv()

    def span(owner):
        return pl.ds(pl.multiple_of(owner * chunk, chunk), chunk)

    def project(token, shift):
        where = span(group_at(shift))
        left = tok[token, :, where]
        for weight in range(2):
            slot = 2 * token + weight
            acc[slot] += jnp.dot(left, whole[weight, where, :], preferred_element_type=f32)

    def loop(first, last, body):
        def step(index, carry):
            body(index)
            return carry

        lax.fori_loop(first, last, step, 0)

    def project_pair(distance, token_list):
        if distance == reach:
            loop(0, len(token_list), lambda i: project(token_list[0] + i, reach))
        else:
            loop(
                0,
                2 * len(token_list),
                lambda i: project(
                    token_list[0] + lax.div(i, 2), (2 * lax.rem(i, 2) - 1) * distance
                ),
            )

    for order in range(2):
        for weight in (0, 1):
            forward(weight, 2, order)
    token_over(0)
    token_in(0)
    loop(0, 3, lambda i: project(0, i - 1))
    later_started = False
    for step in range(3, reach + 1):
        last = step == reach
        if last:
            token_over(1)
            token_in(1)
            loop(0, 3, lambda i: project(1, i - 1))
            for distance in range(2, reach - 1):
                project_pair(distance, [1])
        for order in range(1 if last else 2):
            for weight in (0, 1):
                forward(weight, step, order)
        if last:
            for order in range(2):
                forward(2, 2, order)
        for weight in (0, 1):
            arrive(weight, step - 1)
        project_pair(step - 1, [0, 1] if last else [0])
    token_over(2)
    for weight in (0, 1):
        arrive(weight, reach)
    project_pair(reach, [0, 1])
    for token in range(2):
        settle(tok.at[token, 0 : 3 * rows], tok_ss.at[token])

    tile = 32

    def early_values(index):
        where = pl.ds(pl.multiple_of(index * tile, tile), tile)
        gate, up = acc[0, where, :], acc[1, where, :]
        sig = jax.nn.sigmoid(gate)
        act = gate * sig
        tok[0, where, 0:width] = (act * up).astype(bf16)
        acc[0, where, :] = up * sig * (1.0 + gate * (1.0 - sig))
        acc[1, where, :] = act

    def later_values(index):
        where = pl.ds(pl.multiple_of(index * tile, tile), tile)
        gate, up = acc[2, where, :], acc[3, where, :]
        tok[1, where, 0:width] = (gate * jax.nn.sigmoid(gate) * up).astype(bf16)

    loop(0, total_rows // tile, later_values)

    def slab_of(index):
        if isinstance(index, int):
            return 2 + index // per_slab, index % per_slab * chunk
        first = pl.multiple_of(lax.rem(index, per_slab) * chunk, chunk)
        return 2 + lax.div(index, per_slab), first

    def partial_sum(index):
        left = tok[2, :, span(group_at(index))]
        place_of, first = slab_of(index)
        acc[place_of, pl.ds(first, chunk), :] = lax.dot_general(
            left, tok[0, :, 0:width], (((0,), (0,)), ((), ())), preferred_element_type=f32
        )

    def own_part(shift, part):
        place_of, first = slab_of((shift + ring) % ring)
        return acc[place_of, pl.ds(pl.multiple_of(first + part * half, half), half), :]

    def near_copy(which, owner):
        return remote(
            near_send.at[which, owner],
            near_recv.at[which, owner],
            near_ss.at[0],
            near_rs.at[which, owner],
            peers[1],
        )

    def far_copy(which, owner):
        return remote(
            far_send.at[which, owner],
            far_recv.at[which, owner],
            far_ss.at[0],
            far_rs.at[0 if which == 0 else 1 + lax.div(owner, 2)],
            peers[2],
        )

    def produce(which, owner, value):
        mine[which, owner, 0] = value[:rows]
        mine[which, owner, 1] = value[2 * rows : 3 * rows]
        near_send[which, owner, 0] = value[rows : 2 * rows].astype(bf16)
        near_send[which, owner, 1] = value[3 * rows :].astype(bf16)
        near_copy(which, owner).start()

    def relay(which, owner):
        near_copy(which, owner).wait_recv()
        mine[which, owner, 0] += near_recv[which, owner, 0].astype(f32)
        far_send[which, owner] = (
            mine[which, owner, 1] + near_recv[which, owner, 1].astype(f32)
        ).astype(bf16)
        far_copy(which, owner).start()

    def finish(which, owner):
        outs[which][:, span(owner)] = (
            mine[which, owner, 0] + far_recv[which, owner].astype(f32)
        ).astype(bf16)

    def finish_later():
        remote(far_send.at[0], far_recv.at[0], far_ss.at[0], far_rs.at[0], peers[2]).wait_recv()
        loop(0, ring, lambda i: finish(0, i))

    def finish_pair(pair):
        part = far_recv.at[1, pl.ds(2 * pair, 2)]
        slot = far_rs.at[1 + pair]
        remote(part, part, slot, slot, peers[2]).wait_recv()
        finish(1, 2 * pair)
        finish(1, 2 * pair + 1)

    last_slab = acc.shape[0] - 1

    def output_step(shift):
        owner = group_at(shift)
        produce(0, owner, contract_last(tok[1, :, 0:width], whole[2, span(owner), :]))

    def hidden_step(shift):
        where = span(group_at(shift))
        acc[last_slab] += jnp.dot(
            tok[2, :, where], whole[2, where, :], preferred_element_type=f32
        )

    moved = {}

    def piece_rows(piece):
        return pl.ds(pl.multiple_of((low if piece else 1 - low) * depth, depth), depth)

    def fold(way, step, order, add=True, piece=None):
        part = halves[way][order]
        shift = (reach + 1 - step) * (1 if way == 0 else -1)
        where = slice(None) if piece is None else piece_rows(piece)
        slot = travel.at[way, step - 1, order, where, :]
        if piece is None:
            mine_part = own_part(shift, part)
        else:
            place_of, first = slab_of((shift + ring) % ring)
            member = low if piece else 1 - low
            first = pl.multiple_of(first + part * half + member * depth, depth)
            mine_part = acc[place_of, pl.ds(first, depth), :]
        if add:
            copies = moved[way, step - 1, order]
            for copy in copies if piece is None else copies[piece : piece + 1]:
                copy.wait_recv()
            slot[...] = (slot[...].astype(f32) + mine_part).astype(bf16)
        else:
            slot[...] = mine_part.astype(bf16)

    slots = {}

    def sum_slot(*key):
        return slots.setdefault(key, len(slots))

    def pass_on(way, step, order, pieces=(None,)):
        for piece in pieces:
            where = slice(None) if piece is None else piece_rows(piece)
            moved.setdefault((way, step, order), []).append(
                begin(
                    remote(
                        travel.at[way, step - 1, order, where, :],
                        travel.at[way, step, order, where, :],
                        sum_ss.at[0],
                        sum_rs.at[sum_slot(way, step, order, piece)],
                        around[way],
                    )
                )
            )

    def grads(index):
        where = pl.ds(pl.multiple_of(index * tile, tile), tile)
        hidden = acc[last_slab, where, :]
        tok[0, where, width : 2 * width] = (hidden * acc[0, where, :]).astype(bf16)
        tok[1, where, width : 2 * width] = (hidden * acc[1, where, :]).astype(bf16)

    def input_step(owner):
        where = span(owner)
        produce(
            1,
            owner,
            contract_last(tok[0, :, width : 2 * width], whole[0, where, :])
            + contract_last(tok[1, :, width : 2 * width], whole[1, where, :]),
        )

        @pl.when(owner > 0)
        def _():
            relay(1, owner - 1)

    def both(distance, body):
        loop(0, 2, lambda i: body((2 * i - 1) * distance))

    def relay_at(shift):
        relay(0, group_at(shift))

    def output_near(index):
        output_step(index - 1)

        @pl.when(index > 0)
        def _():
            relay_at(index - 2)

    def output_pair(distance):
        both(distance, output_step)
        both(distance, relay_at)

    loop(0, 3, output_near)
    forward(2, 3, 0)
    loop(0, total_rows // tile, early_values)
    relay_at(1)
    token_in(2)
    loop(reach - 1, reach + 2, partial_sum)
    loop(0, 2, lambda i: hidden_step(i - 1))
    forward(2, 3, 1)
    arrive(2, 2)
    output_pair(2)
    forward(2, reach, 0)
    for way in range(2):
        fold(way, 1, 1, False)
        pass_on(way, 1, 1, (None,) if way else (0, 1))
        fold(way, 2, 0, False)
        pass_on(way, 2, 0, (None,) if way else (0,))

    def step_piece(step, order, piece):
        fold(0, step, order, True, piece)
        pass_on(0, step, order, (piece,))

    hidden_step(1)
    both(2, hidden_step)
    loop(0, ring - 3, lambda i: partial_sum(lax.rem(reach + 2 + i, ring)))
    arrive(2, reach - 1)
    output_pair(reach - 1)
    both(reach - 1, hidden_step)
    arrive(2, reach)
    output_step(reach)
    hidden_step(reach)
    loop(0, total_rows // tile, grads)
    step_piece(2, 1, 0)
    relay_at(reach)
    loop(0, ring // 4, input_step)
    step_piece(2, 1, 1)
    pass_on(0, 2, 0, (1,))
    fold(1, 2, 1)
    pass_on(1, 2, 1)
    loop(ring // 4, ring - 2, input_step)
    step_piece(3, 1, 0)
    fold(1, 3, 0)
    pass_on(1, 3, 0)
    loop(ring - 2, ring, input_step)
    step_piece(3, 1, 1)
    step_piece(3, 0, 0)
    relay(1, ring - 1)
    finish_later()
    step_piece(3, 0, 1)
    fold(1, 3, 1)
    pass_on(1, 3, 1)
    loop(0, ring // 4, finish_pair)
    step_piece(4, 1, 0)
    step_piece(4, 1, 1)
    fold(1, 4, 0)
    pass_on(1, 4, 0, (0, 1))
    finish_pair(ring // 4)
    step_piece(4, 0, 0)
    step_piece(4, 0, 1)
    fold(1, 4, 1)
    pass_on(1, 4, 1, (0, 1))
    def trade(piece, member):
        first = pl.multiple_of(member * depth, depth)
        return begin(
            remote(
                trade_send.at[pl.ds(first, depth), :],
                trade_recv.at[piece - 1],
                trade_ss.at[0],
                trade_rs.at[piece - 1],
                peers[piece],
            )
        )

    def across(member):
        return pl.ds(pl.multiple_of(member * width, width), width)

    def collect(piece):
        trades[piece].wait_recv()
        there = across(relative[piece])
        sum_out[:, there] = sum_ref[:, there] + trade_recv[piece - 1].astype(f32) * factor

    place_of, first = slab_of(0)

    def total(part, orders, piece):
        where = piece_rows(piece)
        member = low if piece else 1 - low
        mine_rows = pl.ds(pl.multiple_of(first + part * half + member * depth, depth), depth)
        result = acc[place_of, mine_rows, :]
        for way in range(2):
            moved[way, reach, orders[way]][piece].wait_recv()
            result = result + travel[way, reach, orders[way], where, :].astype(f32)
        return result

    trades = {}

    def give(piece, part, orders, index):
        first_row = pl.multiple_of(relative[piece] * depth, depth)
        trade_send[pl.ds(first_row, depth), :] = total(part, orders, index).astype(bf16)
        trades[piece] = trade(piece, relative[piece])

    give(3, 1 - high, (1, 0), 0)
    loop(ring // 4 + 1, ring // 2, finish_pair)
    give(2, 1 - high, (1, 0), 1)
    give(1, high, (0, 1), 0)
    collect(3)
    sum_out[:, across(lane)] = sum_ref[:, across(lane)] + total(high, (0, 1), 1) * factor
    collect(2)
    collect(1)

    for weight in range(3):
        settle(whole.at[weight, 0 : 2 * (2 * reach - 1) * half], ring_ss.at[weight])
    settle(whole.at[0, 0 : 9 * depth], quad_ss.at[0])
    settle(tok.at[2, 0 : 3 * rows], tok_ss.at[2])
    settle(near_send, near_ss.at[0])
    settle(far_send, far_ss.at[0])
    settle(whole.at[0, 0 : 2 * (2 * reach - 1) * half], sum_ss.at[0])
    settle(trade_recv, trade_ss.at[0])


def deliver_kernel(*refs):
    sources, targets, done = refs[:3], refs[3:6], refs[6]
    copies = []
    for index, (source, target) in enumerate(zip(sources, targets)):
        size = source.shape[0] // PIECES
        for piece in range(PIECES):
            where = pl.ds(piece * size, size)
            copies.append(
                pltpu.make_async_copy(
                    source.at[where, :], target.at[where, :], done.at[index, piece]
                )
            )
    for copy in copies:
        copy.start()
    for copy in copies:
        copy.wait()


def fused_shards(
    later_input, earlier_input, cotangent, gate_weight, up_weight, down_weight, down_grad_sum
):
    ring = lax.axis_size("fs") // QUAD
    rows, model = later_input.shape
    depth, hidden = gate_weight.shape
    width, chunk, total_rows = hidden // QUAD, QUAD * depth, QUAD * rows
    reach = ring // 2
    slabs = 2 + max(2, pl.cdiv(ring, total_rows // chunk)) + 1
    dma = pltpu.SemaphoreType.DMA
    bf16, f32 = jnp.bfloat16, jnp.float32
    vmem, anywhere = pl.BlockSpec(memory_space=pltpu.VMEM), pl.BlockSpec(memory_space=pl.ANY)
    factor = (rows * lax.axis_size("fs")) ** (-0.5)
    shapes = [
        (later_input.shape, bf16),
        (earlier_input.shape, bf16),
        (down_grad_sum.shape, f32),
    ]
    results = pl.pallas_call(
            functools.partial(fused_kernel, ring, factor),
            out_shape=[pltpu.VMEM(*shape) for shape in shapes],
            in_specs=[anywhere] * 7,
            out_specs=[vmem] * 3,
            scratch_shapes=[
                pltpu.VMEM((3, depth, hidden), bf16),
                pltpu.VMEM((depth, hidden), f32),
                pltpu.VMEM((3, model, width), bf16),
                pltpu.VMEM((3, total_rows, model), bf16),
                pltpu.VMEM((slabs, total_rows, width), f32),
                pltpu.VMEM((2, ring, 2, rows, chunk), f32),
                pltpu.VMEM((2, ring, 2, rows, chunk), bf16),
                pltpu.VMEM((2, ring, 2, rows, chunk), bf16),
                pltpu.VMEM((2, ring, rows, chunk), bf16),
                pltpu.VMEM((2, ring, rows, chunk), bf16),
                pltpu.VMEM((2, reach + 1, 2, 2 * depth, width), bf16),
                pltpu.VMEM((chunk, width), bf16),
                pltpu.VMEM((3, depth, width), bf16),
                dma((1,)),
                dma((3, 3)),
                dma((3, 2, 2)),
                dma((3,)),
                dma((2, 2, reach - 1, 2)),
                dma((3,)),
                dma((3, 2)),
                dma((1,)),
                dma((2, ring)),
                dma((1,)),
                dma((1 + ring // 2,)),
                dma((1,)),
                dma((6 * reach - 1,)),
                dma((1,)),
                dma((3,)),
                dma((6,)),
            ],
            compiler_params=pltpu.CompilerParams(
                collective_id=0, has_side_effects=True, vmem_limit_bytes=62_000_000
            ),
        )(
            earlier_input,
            later_input,
            cotangent,
            gate_weight,
            up_weight,
            down_weight,
            down_grad_sum,
        )
    return tuple(
        pl.pallas_call(
            deliver_kernel,
            out_shape=[jax.ShapeDtypeStruct(*shape) for shape in shapes],
            in_specs=[vmem] * 3,
            out_specs=[anywhere] * 3,
            scratch_shapes=[dma((3, PIECES))],
            compiler_params=pltpu.CompilerParams(vmem_limit_bytes=1_000_000),
        )(*(pltpu.with_memory_space_constraint(value, pltpu.VMEM) for value in results))
    )


def fits(mesh):
    return mesh.shape["tp"] == 1 and mesh.shape["fs"] == 8 * QUAD


def solution(mesh):
    in_specs = (
        P(("fs", "tp"), None),
        P(("fs", "tp"), None),
        P(("fs", "tp"), None),
        P("fs", "tp"),
        P("fs", "tp"),
        P("fs", "tp"),
        P("fs", "tp"),
    )
    out_specs = (P(("fs", "tp"), None), P(("fs", "tp"), None), P("fs", "tp"))
    body = fused_shards if fits(mesh) else shards
    return jax.shard_map(body, mesh=mesh, in_specs=in_specs, out_specs=out_specs, check_vma=False)
```

```python
import functools

import jax
import jax.numpy as jnp
from jax import lax
from jax.experimental import pallas as pl
from jax.experimental.pallas import tpu as pltpu
from jax.sharding import PartitionSpec as P

QUAD = 4
PIECES = 1


def contract_last(leading, trailing):
    return lax.dot_general(
        leading, trailing, (((1,), (1,)), ((), ())), preferred_element_type=jnp.float32
    )


def add_parts(received, group):
    pieces = received.reshape(group, received.shape[0] // group, received.shape[1])
    return jnp.sum(pieces.astype(jnp.float32), axis=0).astype(jnp.bfloat16)


def shards(
    later_input, earlier_input, cotangent, gate_weight, up_weight, down_weight, down_grad_sum
):
    group = lax.axis_size("tp")
    later_rows, early_rows, grad_rows = (
        lax.all_gather(later_input, "tp", axis=0, tiled=True),
        lax.all_gather(earlier_input, "tp", axis=0, tiled=True),
        lax.all_gather(cotangent, "tp", axis=0, tiled=True),
    )
    columns = later_rows
    gate_later = jnp.dot(
        columns,
        lax.all_gather(gate_weight, "fs", axis=0, tiled=True),
        preferred_element_type=jnp.float32,
    )
    up_later = jnp.dot(
        columns,
        lax.all_gather(up_weight, "fs", axis=0, tiled=True),
        preferred_element_type=jnp.float32,
    )
    hidden_later = (jax.nn.silu(gate_later) * up_later).astype(jnp.bfloat16)
    partials = contract_last(hidden_later, lax.all_gather(down_weight, "fs", axis=0, tiled=True))
    gate_whole, up_whole, down_whole = (
        lax.all_gather(gate_weight, "fs", axis=0, tiled=True),
        lax.all_gather(up_weight, "fs", axis=0, tiled=True),
        lax.all_gather(down_weight, "fs", axis=0, tiled=True),
    )
    output_received = lax.all_to_all(
        partials.astype(jnp.bfloat16), "tp", split_axis=0, concat_axis=0, tiled=True
    )
    later_output = add_parts(output_received, group)
    gate_early = jnp.dot(early_rows, gate_whole, preferred_element_type=jnp.float32)
    up_early = jnp.dot(early_rows, up_whole, preferred_element_type=jnp.float32)
    sigmoid_gate = jax.nn.sigmoid(gate_early)
    activated = gate_early * sigmoid_gate
    hidden_early = (activated * up_early).astype(jnp.bfloat16)
    grad_hidden = jnp.dot(grad_rows, down_whole, preferred_element_type=jnp.float32)
    grad_gate = (
        grad_hidden * up_early * sigmoid_gate * (1.0 + gate_early * (1.0 - sigmoid_gate))
    ).astype(jnp.bfloat16)
    grad_up = (grad_hidden * activated).astype(jnp.bfloat16)
    input_partial = contract_last(grad_gate, gate_whole) + contract_last(grad_up, up_whole)
    input_received = lax.all_to_all(
        input_partial.astype(jnp.bfloat16), "tp", split_axis=0, concat_axis=0, tiled=True
    )
    earlier_grad_input = add_parts(input_received, group)
    columns = grad_rows
    summed = lax.psum_scatter(
        lax.dot_general(
            columns, hidden_early, (((0,), (0,)), ((), ())), preferred_element_type=jnp.float32
        ),
        "fs",
        scatter_dimension=0,
        tiled=True,
    )
    factor = (later_rows.shape[0] * lax.axis_size("fs")) ** (-0.5)
    return (later_output, earlier_grad_input, down_grad_sum + summed * factor)

def ring_group(place, ring):
    half = lax.div(2 * place, ring)
    return 2 * place * (1 - half) + (2 * (ring - 1 - place) + 1) * half


def ring_place(group, ring):
    odd = lax.rem(group, 2)
    return lax.div(group, 2) * (1 - odd) + (ring - 1 - lax.div(group, 2)) * odd


def fused_kernel(ring, factor, *refs):
    token_refs, weight_inputs, sum_input = refs[:3], refs[3:6], refs[6]
    outs, sum_out = refs[7:9], refs[9]
    (staged, sum_ref, whole, tok, acc, mine, near_send, near_recv, far_send, far_recv, travel,
     trade_send, trade_recv) = refs[10:23]
    (quad_ss, quad_rs, first_rs, ring_ss, ring_rs, tok_ss, tok_rs, near_ss, near_rs,
     far_ss, far_rs, sum_ss, sum_rs, trade_ss, trade_rs, local_sem) = refs[23:]
    weight_refs = [staged.at[weight] for weight in range(3)]
    bf16, f32 = jnp.bfloat16, jnp.float32
    me = lax.axis_index("fs")
    group, lane = lax.div(me, QUAD), lax.rem(me, QUAD)
    low, high = lax.rem(lane, 2), lax.div(lane, 2)
    relative = [lane, lane + 1 - 2 * low, lane + 2 - 4 * high, QUAD - 1 - lane]
    peers = [group * QUAD + other for other in relative]
    place = ring_place(group, ring)

    def group_at(shift):
        return ring_group(lax.rem(place + shift + ring, ring), ring)

    around = [group_at(1) * QUAD + lane, group_at(-1) * QUAD + lane]
    depth = weight_refs[0].shape[0]
    width = whole.shape[2]
    chunk, half = QUAD * depth, 2 * depth
    rows = token_refs[0].shape[0]
    total_rows = tok.shape[1]
    reach = ring // 2
    per_slab = total_rows // chunk
    halves = [[high, 1 - high], [1 - high, high]]

    barrier = pltpu.get_barrier_semaphore()
    for other in peers[1:] + around:
        pl.semaphore_signal(
            barrier, inc=1, device_id={"fs": other}, device_id_type=pl.DeviceIdType.MESH
        )
    staging = [
        pltpu.make_async_copy(weight_inputs[weight], staged.at[weight], local_sem.at[2 + weight])
        for weight in range(3)
    ]
    staging.append(pltpu.make_async_copy(sum_input, sum_ref, local_sem.at[5]))
    for copy in staging:
        copy.start()
    pl.semaphore_wait(barrier, QUAD + 1)

    def remote(source, target, send, recv, other):
        return pltpu.make_async_remote_copy(
            src_ref=source,
            dst_ref=target,
            send_sem=send,
            recv_sem=recv,
            device_id={"fs": other},
            device_id_type=pl.DeviceIdType.MESH,
        )

    def slab(weight, owner, member):
        first = pl.multiple_of((owner * QUAD + member) * depth, depth)
        return whole.at[weight, pl.ds(first, depth), :]

    def columns(weight, member):
        return weight_refs[weight].at[:, pl.ds(pl.multiple_of(member * width, width), width)]

    def half_slab(weight, owner, part):
        first = pl.multiple_of(owner * chunk + part * half, half)
        return whole.at[weight, pl.ds(first, half), :]

    def begin(copy):
        copy.start()
        return copy

    def settle(part, send):
        remote(part, part, send, send, peers[1]).wait_send()

    quad, first_hop, hop, tokens = {}, {}, {}, {}

    def hop_first(weight, piece):
        for way in range(2):
            target = slab(weight, group, relative[piece])
            first_hop[weight, way, piece] = begin(
                remote(
                    columns(weight, lane) if piece == 0 else target,
                    target,
                    ring_ss.at[0],
                    first_rs.at[weight, way, 0 if piece < 2 else 1],
                    around[way],
                )
            )

    for weight in range(3):
        staging[weight].wait()
        for far in (1, 3, 2):
            quad[weight, far] = begin(
                remote(
                    columns(weight, relative[far]),
                    slab(weight, group, lane),
                    quad_ss.at[0],
                    quad_rs.at[weight, min(far - 1, 1)],
                    peers[far],
                )
            )
        if weight < 2:
            hop_first(weight, 0)

    for weight in range(3):
        copy = pltpu.make_async_copy(
            columns(weight, lane), slab(weight, group, lane), local_sem.at[0]
        )
        copy.start()

    def row_block(token, block):
        return tok.at[token, pl.ds(block * rows, rows), :]

    def send_rows(token, source, block, slot, other):
        tokens[token, slot] = begin(
            remote(
                source,
                row_block(token, block),
                tok_ss.at[token],
                tok_rs.at[token, slot % 2],
                other,
            )
        )

    for token in range(3):
        send_rows(token, token_refs[token], 2, 1, peers[2])
        send_rows(token, token_refs[token], 1, 0, peers[1])
        copy = pltpu.make_async_copy(
            token_refs[token], row_block(token, 0), local_sem.at[1]
        )
        copy.start()

    def clear(index, carry):
        acc[index] = jnp.zeros(acc.shape[1:], f32)
        return carry

    lax.fori_loop(0, 4, clear, 0)
    acc[acc.shape[0] - 1] = jnp.zeros(acc.shape[1:], f32)

    for weight in (0, 1):
        quad[weight, 1].wait_recv()
        hop_first(weight, 1)
    hop_first(2, 0)
    quad[2, 1].wait_recv()
    hop_first(2, 1)
    for weight in range(3):
        part = half_slab(weight, group, 1 - high)
        slot = quad_rs.at[weight, 1]
        remote(part, part, slot, slot, peers[1]).wait_recv()
        for way in range(2):
            begin(
                remote(
                    part, part, ring_ss.at[0], first_rs.at[weight, way, 1], around[way]
                )
            )
    staging[3].wait()
    for part, index in ((whole.at[0, 0 : 3 * depth], 0), (tok.at[0, 0 : 3 * rows], 1)):
        pltpu.make_async_copy(part, part, local_sem.at[index]).wait()

    arrived = set()

    def hop_slot(weight, way, step, order):
        return (max(weight - 1, 0) * 2 + way) * (2 * reach - 3) + 2 * (step - 2) + order

    def arrival(weight, way, step, order):
        if step > 1 and weight == 0:
            weight = 1
        if (weight, way, step, order) in arrived:
            return
        arrived.add((weight, way, step, order))
        if step == 1:
            side = 0 if (order == 0) == (way == 0) else 1
            part = half_slab(weight, group_at(-1 if way == 0 else 1), halves[way][order])
            slot = first_rs.at[weight, way, side]
            remote(part, part, slot, slot, peers[1]).wait_recv()
        else:
            part = whole.at[0, 0 : half if weight == 2 else chunk]
            slot = ring_rs.at[hop_slot(weight, way, step, order)]
            remote(part, part, slot, slot, peers[1]).wait_recv()

    def forward(weight, step, order):
        for way in range(2):
            arrival(weight, way, step - 1, order)
            shift = (1 - step) if way == 0 else (step - 1)
            part = half_slab(weight, group_at(shift), halves[way][order])
            hop[weight, way, step, order] = begin(
                remote(
                    part,
                    part,
                    ring_ss.at[0],
                    ring_rs.at[hop_slot(weight, way, step, order)],
                    around[way],
                )
            )

    def arrive(weight, distance):
        for way in range(2):
            for order in range(1 if distance == reach else 2):
                arrival(weight, way, distance, order)

    def token_over(token):
        tokens[token, 1].wait_recv()
        send_rows(token, row_block(token, 2), 3, 2, peers[1])

    def token_in(token):
        part, slot = tok.at[0, 0 : 2 * rows], tok_rs.at[token, 0]
        remote(part, part, slot, slot, peers[1]).wait_recv()

    def span(owner):
        return pl.ds(pl.multiple_of(owner * chunk, chunk), chunk)

    def project(token, shift):
        where = span(group_at(shift))
        left = tok[token, :, where]
        for weight in range(2):
            slot = 2 * token + weight
            acc[slot] += jnp.dot(left, whole[weight, where, :], preferred_element_type=f32)

    def loop(first, last, body):
        def step(index, carry):
            body(index)
            return carry

        lax.fori_loop(first, last, step, 0)

    def project_pair(distance, token_list):
        if distance == reach:
            loop(0, len(token_list), lambda i: project(token_list[0] + i, reach))
        else:
            loop(
                0,
                2 * len(token_list),
                lambda i: project(
                    token_list[0] + lax.div(i, 2), (2 * lax.rem(i, 2) - 1) * distance
                ),
            )

    for order in range(2):
        for weight in (0, 1):
            forward(weight, 2, order)
    token_over(0)
    token_in(0)
    loop(0, 3, lambda i: project(0, i - 1))
    later_started = False
    for step in range(3, reach + 1):
        last = step == reach
        if last:
            token_over(1)
            token_in(1)
            loop(0, 3, lambda i: project(1, i - 1))
            for distance in range(2, reach - 1):
                project_pair(distance, [1])
        for order in range(1 if last else 2):
            for weight in (0, 1):
                forward(weight, step, order)
        if last:
            for order in range(2):
                forward(2, 2, order)
        for weight in (0, 1):
            arrive(weight, step - 1)
        project_pair(step - 1, [0, 1] if last else [0])
    token_over(2)
    for weight in (0, 1):
        arrive(weight, reach)
    project_pair(reach, [0, 1])
    for token in range(2):
        settle(tok.at[token, 0 : 3 * rows], tok_ss.at[token])

    tile = 32

    def early_values(index):
        where = pl.ds(pl.multiple_of(index * tile, tile), tile)
        gate, up = acc[0, where, :], acc[1, where, :]
        sig = jax.nn.sigmoid(gate)
        act = gate * sig
        tok[0, where, 0:width] = (act * up).astype(bf16)
        acc[0, where, :] = up * sig * (1.0 + gate * (1.0 - sig))
        acc[1, where, :] = act

    def later_values(index):
        where = pl.ds(pl.multiple_of(index * tile, tile), tile)
        gate, up = acc[2, where, :], acc[3, where, :]
        tok[1, where, 0:width] = (gate * jax.nn.sigmoid(gate) * up).astype(bf16)

    loop(0, total_rows // tile, later_values)

    def slab_of(index):
        if isinstance(index, int):
            return 2 + index // per_slab, index % per_slab * chunk
        first = pl.multiple_of(lax.rem(index, per_slab) * chunk, chunk)
        return 2 + lax.div(index, per_slab), first

    def partial_sum(index):
        left = tok[2, :, span(group_at(index))]
        place_of, first = slab_of(index)
        acc[place_of, pl.ds(first, chunk), :] = lax.dot_general(
            left, tok[0, :, 0:width], (((0,), (0,)), ((), ())), preferred_element_type=f32
        )

    def own_part(shift, part):
        place_of, first = slab_of((shift + ring) % ring)
        return acc[place_of, pl.ds(pl.multiple_of(first + part * half, half), half), :]

    def near_copy(which, owner):
        return remote(
            near_send.at[which, owner],
            near_recv.at[which, owner],
            near_ss.at[0],
            near_rs.at[which, owner],
            peers[1],
        )

    def far_copy(which, owner):
        return remote(
            far_send.at[which, owner],
            far_recv.at[which, owner],
            far_ss.at[0],
            far_rs.at[0 if which == 0 else 1 + lax.div(owner, 2)],
            peers[2],
        )

    def produce(which, owner, value):
        mine[which, owner, 0] = value[:rows]
        mine[which, owner, 1] = value[2 * rows : 3 * rows]
        near_send[which, owner, 0] = value[rows : 2 * rows].astype(bf16)
        near_send[which, owner, 1] = value[3 * rows :].astype(bf16)
        near_copy(which, owner).start()

    def relay(which, owner):
        near_copy(which, owner).wait_recv()
        mine[which, owner, 0] += near_recv[which, owner, 0].astype(f32)
        far_send[which, owner] = (
            mine[which, owner, 1] + near_recv[which, owner, 1].astype(f32)
        ).astype(bf16)
        far_copy(which, owner).start()

    def finish(which, owner):
        outs[which][:, span(owner)] = (
            mine[which, owner, 0] + far_recv[which, owner].astype(f32)
        ).astype(bf16)

    def finish_later():
        remote(far_send.at[0], far_recv.at[0], far_ss.at[0], far_rs.at[0], peers[2]).wait_recv()
        loop(0, ring, lambda i: finish(0, i))

    def finish_pair(pair):
        part = far_recv.at[1, pl.ds(2 * pair, 2)]
        slot = far_rs.at[1 + pair]
        remote(part, part, slot, slot, peers[2]).wait_recv()
        finish(1, 2 * pair)
        finish(1, 2 * pair + 1)

    last_slab = acc.shape[0] - 1

    def output_step(shift):
        owner = group_at(shift)
        produce(0, owner, contract_last(tok[1, :, 0:width], whole[2, span(owner), :]))

    def hidden_step(shift):
        where = span(group_at(shift))
        acc[last_slab] += jnp.dot(
            tok[2, :, where], whole[2, where, :], preferred_element_type=f32
        )

    moved = {}

    def piece_rows(piece):
        return pl.ds(pl.multiple_of((low if piece else 1 - low) * depth, depth), depth)

    def fold(way, step, order, add=True, piece=None):
        part = halves[way][order]
        shift = (reach + 1 - step) * (1 if way == 0 else -1)
        where = slice(None) if piece is None else piece_rows(piece)
        slot = travel.at[way, step - 1, order, where, :]
        if piece is None:
            mine_part = own_part(shift, part)
        else:
            place_of, first = slab_of((shift + ring) % ring)
            member = low if piece else 1 - low
            first = pl.multiple_of(first + part * half + member * depth, depth)
            mine_part = acc[place_of, pl.ds(first, depth), :]
        if add:
            copies = moved[way, step - 1, order]
            for copy in copies if piece is None else copies[piece : piece + 1]:
                copy.wait_recv()
            slot[...] = (slot[...].astype(f32) + mine_part).astype(bf16)
        else:
            slot[...] = mine_part.astype(bf16)

    slots = {}

    def sum_slot(*key):
        return slots.setdefault(key, len(slots))

    def pass_on(way, step, order, pieces=(None,)):
        for piece in pieces:
            where = slice(None) if piece is None else piece_rows(piece)
            moved.setdefault((way, step, order), []).append(
                begin(
                    remote(
                        travel.at[way, step - 1, order, where, :],
                        travel.at[way, step, order, where, :],
                        sum_ss.at[0],
                        sum_rs.at[sum_slot(way, step, order, piece)],
                        around[way],
                    )
                )
            )

    def grads(index):
        where = pl.ds(pl.multiple_of(index * tile, tile), tile)
        hidden = acc[last_slab, where, :]
        tok[0, where, width : 2 * width] = (hidden * acc[0, where, :]).astype(bf16)
        tok[1, where, width : 2 * width] = (hidden * acc[1, where, :]).astype(bf16)

    def input_step(owner):
        where = span(owner)
        produce(
            1,
            owner,
            contract_last(tok[0, :, width : 2 * width], whole[0, where, :])
            + contract_last(tok[1, :, width : 2 * width], whole[1, where, :]),
        )

        @pl.when(owner > 0)
        def _():
            relay(1, owner - 1)

    def both(distance, body):
        loop(0, 2, lambda i: body((2 * i - 1) * distance))

    def relay_at(shift):
        relay(0, group_at(shift))

    def output_near(index):
        output_step(index - 1)

        @pl.when(index > 0)
        def _():
            relay_at(index - 2)

    def output_pair(distance):
        both(distance, output_step)
        both(distance, relay_at)

    loop(0, 3, output_near)
    forward(2, 3, 0)
    loop(0, total_rows // tile, early_values)
    relay_at(1)
    token_in(2)
    loop(reach - 1, reach + 2, partial_sum)
    loop(0, 2, lambda i: hidden_step(i - 1))
    forward(2, 3, 1)
    arrive(2, 2)
    output_pair(2)
    forward(2, reach, 0)
    for way in range(2):
        fold(way, 1, 1, False)
        pass_on(way, 1, 1, (None,) if way else (0, 1))
        fold(way, 2, 0, False)
        pass_on(way, 2, 0, (None,) if way else (0,))

    def step_piece(step, order, piece):
        fold(0, step, order, True, piece)
        pass_on(0, step, order, (piece,))

    hidden_step(1)
    both(2, hidden_step)
    loop(0, ring - 3, lambda i: partial_sum(lax.rem(reach + 2 + i, ring)))
    arrive(2, reach - 1)
    output_pair(reach - 1)
    both(reach - 1, hidden_step)
    arrive(2, reach)
    output_step(reach)
    hidden_step(reach)
    loop(0, total_rows // tile, grads)
    step_piece(2, 1, 0)
    relay_at(reach)
    loop(0, ring // 4, input_step)
    step_piece(2, 1, 1)
    pass_on(0, 2, 0, (1,))
    fold(1, 2, 1)
    pass_on(1, 2, 1)
    loop(ring // 4, ring - 2, input_step)
    step_piece(3, 1, 0)
    fold(1, 3, 0)
    pass_on(1, 3, 0)
    loop(ring - 2, ring, input_step)
    step_piece(3, 1, 1)
    step_piece(3, 0, 0)
    relay(1, ring - 1)
    finish_later()
    step_piece(3, 0, 1)
    fold(1, 3, 1)
    pass_on(1, 3, 1)
    loop(0, ring // 4, finish_pair)
    step_piece(4, 1, 0)
    step_piece(4, 1, 1)
    fold(1, 4, 0)
    pass_on(1, 4, 0, (0, 1))
    finish_pair(ring // 4)
    step_piece(4, 0, 0)
    step_piece(4, 0, 1)
    fold(1, 4, 1)
    pass_on(1, 4, 1, (0, 1))
    def trade(piece, member):
        first = pl.multiple_of(member * depth, depth)
        return begin(
            remote(
                trade_send.at[pl.ds(first, depth), :],
                trade_recv.at[piece - 1],
                trade_ss.at[0],
                trade_rs.at[piece - 1],
                peers[piece],
            )
        )

    def across(member):
        return pl.ds(pl.multiple_of(member * width, width), width)

    def collect(piece):
        trades[piece].wait_recv()
        there = across(relative[piece])
        sum_out[:, there] = sum_ref[:, there] + trade_recv[piece - 1].astype(f32) * factor

    place_of, first = slab_of(0)

    def total(part, orders, piece):
        where = piece_rows(piece)
        member = low if piece else 1 - low
        mine_rows = pl.ds(pl.multiple_of(first + part * half + member * depth, depth), depth)
        result = acc[place_of, mine_rows, :]
        for way in range(2):
            moved[way, reach, orders[way]][piece].wait_recv()
            result = result + travel[way, reach, orders[way], where, :].astype(f32)
        return result

    trades = {}

    def give(piece, part, orders, index):
        first_row = pl.multiple_of(relative[piece] * depth, depth)
        trade_send[pl.ds(first_row, depth), :] = total(part, orders, index).astype(bf16)
        trades[piece] = trade(piece, relative[piece])

    give(3, 1 - high, (1, 0), 0)
    loop(ring // 4 + 1, ring // 2, finish_pair)
    give(2, 1 - high, (1, 0), 1)
    give(1, high, (0, 1), 0)
    collect(3)
    sum_out[:, across(lane)] = sum_ref[:, across(lane)] + total(high, (0, 1), 1) * factor
    collect(2)
    collect(1)

    settle(whole.at[:, 0 : 2 * (2 * reach - 1) * half], ring_ss.at[0])
    settle(whole.at[0, 0 : 9 * depth], quad_ss.at[0])
    settle(tok.at[2, 0 : 3 * rows], tok_ss.at[2])
    settle(near_send, near_ss.at[0])
    settle(far_send, far_ss.at[0])
    settle(whole.at[0, 0 : 2 * (2 * reach - 1) * half], sum_ss.at[0])
    settle(trade_recv, trade_ss.at[0])


def deliver_kernel(*refs):
    sources, targets, done = refs[:3], refs[3:6], refs[6]
    copies = []
    for index, (source, target) in enumerate(zip(sources, targets)):
        size = source.shape[0] // PIECES
        for piece in range(PIECES):
            where = pl.ds(piece * size, size)
            copies.append(
                pltpu.make_async_copy(
                    source.at[where, :], target.at[where, :], done.at[index, piece]
                )
            )
    for copy in copies:
        copy.start()
    for copy in copies:
        copy.wait()


def fused_shards(
    later_input, earlier_input, cotangent, gate_weight, up_weight, down_weight, down_grad_sum
):
    ring = lax.axis_size("fs") // QUAD
    rows, model = later_input.shape
    depth, hidden = gate_weight.shape
    width, chunk, total_rows = hidden // QUAD, QUAD * depth, QUAD * rows
    reach = ring // 2
    slabs = 2 + max(2, pl.cdiv(ring, total_rows // chunk)) + 1
    dma = pltpu.SemaphoreType.DMA
    bf16, f32 = jnp.bfloat16, jnp.float32
    vmem, anywhere = pl.BlockSpec(memory_space=pltpu.VMEM), pl.BlockSpec(memory_space=pl.ANY)
    factor = (rows * lax.axis_size("fs")) ** (-0.5)
    shapes = [
        (later_input.shape, bf16),
        (earlier_input.shape, bf16),
        (down_grad_sum.shape, f32),
    ]
    results = pl.pallas_call(
            functools.partial(fused_kernel, ring, factor),
            out_shape=[pltpu.VMEM(*shape) for shape in shapes],
            in_specs=[anywhere] * 7,
            out_specs=[vmem] * 3,
            scratch_shapes=[
                pltpu.VMEM((3, depth, hidden), bf16),
                pltpu.VMEM((depth, hidden), f32),
                pltpu.VMEM((3, model, width), bf16),
                pltpu.VMEM((3, total_rows, model), bf16),
                pltpu.VMEM((slabs, total_rows, width), f32),
                pltpu.VMEM((2, ring, 2, rows, chunk), f32),
                pltpu.VMEM((2, ring, 2, rows, chunk), bf16),
                pltpu.VMEM((2, ring, 2, rows, chunk), bf16),
                pltpu.VMEM((2, ring, rows, chunk), bf16),
                pltpu.VMEM((2, ring, rows, chunk), bf16),
                pltpu.VMEM((2, reach + 1, 2, 2 * depth, width), bf16),
                pltpu.VMEM((chunk, width), bf16),
                pltpu.VMEM((3, depth, width), bf16),
                dma((1,)),
                dma((3, 2)),
                dma((3, 2, 2)),
                dma((1,)),
                dma((4 * (2 * reach - 3),)),
                dma((3,)),
                dma((3, 2)),
                dma((1,)),
                dma((2, ring)),
                dma((1,)),
                dma((1 + ring // 2,)),
                dma((1,)),
                dma((6 * reach - 1,)),
                dma((1,)),
                dma((3,)),
                dma((6,)),
            ],
            compiler_params=pltpu.CompilerParams(
                collective_id=0, has_side_effects=True, vmem_limit_bytes=62_000_000
            ),
        )(
            earlier_input,
            later_input,
            cotangent,
            gate_weight,
            up_weight,
            down_weight,
            down_grad_sum,
        )
    return tuple(
        pl.pallas_call(
            deliver_kernel,
            out_shape=[jax.ShapeDtypeStruct(*shape) for shape in shapes],
            in_specs=[vmem] * 3,
            out_specs=[anywhere] * 3,
            scratch_shapes=[dma((3, PIECES))],
            compiler_params=pltpu.CompilerParams(vmem_limit_bytes=1_000_000),
        )(*(pltpu.with_memory_space_constraint(value, pltpu.VMEM) for value in results))
    )


def fits(mesh):
    return mesh.shape["tp"] == 1 and mesh.shape["fs"] == 8 * QUAD


def solution(mesh):
    in_specs = (
        P(("fs", "tp"), None),
        P(("fs", "tp"), None),
        P(("fs", "tp"), None),
        P("fs", "tp"),
        P("fs", "tp"),
        P("fs", "tp"),
        P("fs", "tp"),
    )
    out_specs = (P(("fs", "tp"), None), P(("fs", "tp"), None), P("fs", "tp"))
    body = fused_shards if fits(mesh) else shards
    return jax.shard_map(body, mesh=mesh, in_specs=in_specs, out_specs=out_specs, check_vma=False)
```
